512 devices in a mesh: grp: 2 (over y), tp: 32 (over z), dp: 8 (over x, core).
Axes of the slice: x: 4, y: 2, z: 32, core: 2. Of those that a mesh axis runs over, the one named last changes fastest.
The devices are a block of a 4x8x32 slice.
Arguments:
- residual_token_input: bfloat16 [128, 4096], P('grp', 'dp'), parts along dimension 0, may hold values from -64 to 64
- sequence_token_count: int32 [128], P(('grp', 'dp')), parts along dimension 0, may hold values from 1 to 16, 256 in all
- input_norm_gain: float32 [2, 4096], P(None, 'dp'), may hold values from 0.1 to 1.9
- value_projection: bfloat16 [2, 4096, 4096], P(None, 'dp', 'tp'), may hold values from -0.09375 to 0.09375
- input_key_projection: bfloat16 [2, 4096, 4096], P(None, 'dp', 'tp'), may hold values from -0.09375 to 0.09375
- readout_key_projection: bfloat16 [2, 4096, 4096], P(None, 'dp', 'tp'), may hold values from -0.09375 to 0.09375
- gate_projection: bfloat16 [2, 4096, 4096], P(None, 'dp', 'tp'), may hold values from -0.09375 to 0.09375
- step_size_projection: bfloat16 [2, 4096, 64], P(None, 'dp'), may hold values from -0.09375 to 0.09375
- convolution_weights: bfloat16 [2, 5, 3, 4096], P(None, None, None, 'tp'), may hold values from -2.5 to 2.5
- convolution_history: bfloat16 [2, 128, 4, 3, 4096], P(None, ('grp', 'dp'), None, None, 'tp'), parts along dimension 1, may hold values from -6 to 6
- step_size_bias: float32 [2, 64], P(None, 'tp'), may hold values from -4.6 to -1.5
- head_decay_logarithm: float32 [2, 64], P(None, 'tp'), may hold values from 0 to 2.77
- direct_path_gain: float32 [2, 64], P(None, 'tp'), may hold values from 0.1 to 1.9
- extra_decay_logarithm: float32 [2, 128, 64], P(None, ('grp', 'dp'), 'tp'), parts along dimension 1, may hold values from -0.7 to 0
- recurrent_state: float32 [2, 128, 64, 64, 128], P(None, ('grp', 'dp'), 'tp'), parts along dimension 1, may hold values from -1.5 to 1.5
- output_norm_gain: float32 [2, 4096], P(None, 'tp'), may hold values from 0.1 to 1.9
- output_projection: bfloat16 [2, 4096, 4096], P(None, 'tp', 'dp'), may hold values from -0.09375 to 0.09375
Outputs:
- hidden_out: bfloat16 [128, 4096], P(('grp', 'tp'), 'dp'), parts along dimension 0
- state_out: float32 [2, 128, 64, 64, 128], P(None, ('grp', 'dp'), 'tp'), parts along dimension 1
- window_out: bfloat16 [2, 128, 4, 3, 4096], P(None, ('grp', 'dp'), None, None, 'tp'), parts along dimension 1
The draws below stay inside these ranges and needn't reach their ends.
There are 2 independent parts, one for each index of `grp`. The reference program is written for one: setup_inputs(seed, part) draws one part's arguments, and reference() takes and returns one part's arrays. A program takes and returns all parts, laid end to end along the dimension named above; an argument that names none is the same for every part. Nothing has to cross between parts.
Inputs may be any that keep to these rules, and one draw needn't show every extreme that they name: `sequence_token_count`: tokens already in each sequence before this step.
All inputs are finite; a program needn't handle non-finite values. No bound on the sum of `sequence_token_count` on one device may be relied on, other than what follows from the above.
Results may differ from the reference program's by a relative error of at most 0.015.
Values may be sent and summed in bfloat16 or wider, within the bound.
A program may use at most 64 MiB of HBM per device.

```python
import math
import jax
import jax.numpy as jnp
import numpy as np
from jax import lax

D = 4096
HEADS = 64
HEAD_DIM = 64
GROUPS = 32
STATE = 128
CONV_W = 5
LAYERS = 2
MOST_LEN = 16
BATCH = 64
CHANNELS = 4096


def draw_residual_token_input(key, part):
    key_base, key_rows, key_cols = jax.random.split(key, 3)
    base_draw = jax.random.truncated_normal(key_base, -6.0, 6.0, (BATCH, D), jnp.float32)
    row_scale = jnp.exp(jax.random.uniform(key_rows, (BATCH, 1), jnp.float32, math.log(0.3), math.log(3.0)))
    ramp_factor = 3.0
    position = jnp.arange(D, dtype=jnp.float32) / (D - 1) - 0.5
    col_scale = jnp.exp(position * math.log(ramp_factor) + jax.random.uniform(key_cols, (D,), jnp.float32, -0.6, 0.6))
    return (base_draw * row_scale * col_scale[None, :]).astype(jnp.bfloat16)


def draw_extra_decay_logarithm(key, part):
    key_hit, key_loss = jax.random.split(key)
    shape_all = (LAYERS, BATCH, HEADS)
    struck = jax.random.uniform(key_hit, shape_all, jnp.float32) < 0.25
    loss_share = jax.random.uniform(key_loss, shape_all, jnp.float32, 0.2, 0.5)
    return jnp.where(struck, jnp.log(1.0 - loss_share), 0.0).astype(jnp.float32)


def block_scale(own_key, extent, pieces, low, high):
    loudness, own = 1.0, jax.random.fold_in(own_key, 6)
    for axis_at, shards_of in pieces:
        steps = jnp.exp(jax.random.uniform(jax.random.fold_in(own, axis_at), (shards_of,), jnp.float32, low / len(pieces), high / len(pieces)))
        loudness = loudness * jnp.repeat(steps, extent[axis_at] // shards_of).reshape([-1 if axis == axis_at else 1 for axis in range(len(extent))])
    return loudness


def length_profile(count, total, bound, lean):
    portions = [(1 << 20) // math.isqrt(rank ** lean) + 1 for rank in range(2, count + 1)]
    rest, given = total - bound - (count - 1), [1] * (count - 1)
    while rest > 0:
        free = [i for i in range(count - 1) if given[i] < bound]
        mass, remaining = sum([portions[i] for i in free]), rest
        for i in free:
            addition = min(bound - given[i], max(1, remaining * portions[i] // mass), rest)
            given[i] = given[i] + addition
            rest = rest - addition
    return np.array([bound] + given)


def uneven(rng, number_of, total, limit, slope):
    if number_of == 2:
        one = jax.random.randint(rng, (), max(1, total - limit), min(limit, total - 1) + 1)
        return jnp.stack([one, total - one])
    sizes = jnp.asarray(length_profile(number_of, total, limit, slope), jnp.int32)
    twos = (number_of - 1) // 2
    giver, sink = sizes[1:1 + 2 * twos:2], sizes[2:2 + 2 * twos:2]
    margin = jnp.minimum(giver - 1, limit - sink)
    moved = jax.random.randint(jax.random.fold_in(rng, 1), (twos,), 0, 1 << 20) % (margin + 1)
    sizes = sizes.at[1:1 + 2 * twos:2].set(giver - moved).at[2:2 + 2 * twos:2].set(sink + moved)
    return sizes[jax.random.permutation(jax.random.fold_in(rng, 2), number_of)]


def normal_values(stream_key, shape, scale, most, shards=(), kind=jnp.bfloat16):
    level = block_scale(stream_key, shape, shards, -0.22, 0.18) if shards else 1.0
    values = jax.random.normal(stream_key, shape, jnp.float32) * scale * level
    return jnp.minimum(jnp.maximum(values, -most), most).astype(kind)


def setup_inputs(seed: int = 0, part: int = 0) -> dict:
    key_list = jax.random.split(jax.random.key(seed), 18)
    part_keys = jax.random.split(jax.random.fold_in(key_list[17], part), 18)
    return {
        "residual_token_input": draw_residual_token_input(jax.random.fold_in(jax.random.fold_in(key_list[17], part), 71), part),
        "sequence_token_count": uneven(part_keys[1], BATCH, 4 * BATCH, MOST_LEN, 2).astype(jnp.int32),
        "input_norm_gain": jnp.clip(1.0 + 0.18 * jax.random.normal(key_list[2], (LAYERS, D), jnp.float32), 0.1, 1.9),
        "value_projection": normal_values(key_list[3], (LAYERS, D, CHANNELS), D ** -0.5, 0.09375, ((1, 8), (2, 32))),
        "input_key_projection": normal_values(key_list[4], (LAYERS, D, CHANNELS), D ** -0.5, 0.09375, ((1, 8), (2, 32))),
        "readout_key_projection": normal_values(key_list[5], (LAYERS, D, CHANNELS), D ** -0.5, 0.09375, ((1, 8), (2, 32))),
        "gate_projection": normal_values(key_list[6], (LAYERS, D, CHANNELS), D ** -0.5, 0.09375, ((1, 8), (2, 32))),
        "step_size_projection": normal_values(key_list[7], (LAYERS, D, HEADS), D ** -0.5, 0.09375, ((1, 8),)),
        "convolution_weights": normal_values(key_list[8], (LAYERS, CONV_W, 3, CHANNELS), CONV_W ** -0.5, 2.5, ((3, 32),)),
        "convolution_history": normal_values(part_keys[9], (LAYERS, BATCH, CONV_W - 1, 3, CHANNELS), 1.0, 6.0, ((1, 8), (4, 32))),
        "step_size_bias": jnp.clip(-4.6 + 3.1 * jax.random.uniform(key_list[10], (LAYERS, HEADS), jnp.float32) ** block_scale(key_list[10], (LAYERS, HEADS), ((1, 32),), -0.2, 0.2), -4.6, -1.5),
        "head_decay_logarithm": jnp.clip(2.77 * jax.random.uniform(key_list[11], (LAYERS, HEADS), jnp.float32) ** block_scale(key_list[11], (LAYERS, HEADS), ((1, 32),), -0.2, 0.2), 0.0, 2.77),
        "direct_path_gain": jnp.clip(1.0 + 0.18 * jax.random.normal(key_list[12], (LAYERS, HEADS), jnp.float32), 0.1, 1.9),
        "extra_decay_logarithm": draw_extra_decay_logarithm(jax.random.fold_in(jax.random.fold_in(key_list[17], part), 71), part),
        "recurrent_state": normal_values(part_keys[14], (LAYERS, BATCH, HEADS, HEAD_DIM, STATE), 0.1, 1.5, ((1, 8), (2, 32)), jnp.float32),
        "output_norm_gain": jnp.clip(1.0 + 0.18 * jax.random.normal(key_list[15], (LAYERS, CHANNELS), jnp.float32), 0.1, 1.9),
        "output_projection": normal_values(key_list[16], (LAYERS, CHANNELS, D), CHANNELS ** -0.5, 0.09375, ((1, 32), (2, 8))),
    }


EPSILON = 1e-06

def conv_mixed(current, window_layer, taps_layer, lengths_now):
    taps_float = taps_layer.astype(jnp.float32)
    width_back = window_layer.shape[1]
    steps_back = width_back - jnp.arange(width_back, dtype=jnp.int32)
    live_mask = (steps_back[None, :] <= lengths_now[:, None]).astype(jnp.float32)
    earlier = lax.optimization_barrier(jnp.sum(window_layer.astype(jnp.float32) * live_mask[:, :, None, None] * taps_float[None, :width_back], axis=1))
    return jax.nn.silu(earlier + current.astype(jnp.float32) * taps_float[width_back][None])

def state_after_update(layer_recurrent_state, layer_extra_decay, mixer_input_normed, step_size_input, layer_bias_slice, layer_decay_logarithm, layer_direct_gain):
    seq_count, heads_here, head_width, state_width = layer_recurrent_state.shape
    groups_here = mixer_input_normed.shape[2] // state_width
    per_group = heads_here // groups_here
    step_size_value = jax.nn.softplus(step_size_input.astype(jnp.float32) + layer_bias_slice[None])
    decay_factor_current = jnp.exp(-step_size_value * jnp.exp(layer_decay_logarithm)[None] + layer_extra_decay)
    values = mixer_input_normed[:, 0].reshape(seq_count, groups_here, per_group, head_width)
    inkeys = mixer_input_normed[:, 1].reshape(seq_count, groups_here, state_width)
    readkeys = mixer_input_normed[:, 2].reshape(seq_count, groups_here, state_width)
    grouped_state = layer_recurrent_state.reshape(seq_count, groups_here, per_group, head_width, state_width)
    decay_group = decay_factor_current.reshape(seq_count, groups_here, per_group)
    rate_group = step_size_value.reshape(seq_count, groups_here, per_group)
    skip_group = layer_direct_gain.reshape(groups_here, per_group)
    updated_state = decay_group[..., None, None] * grouped_state + (rate_group[..., None] * values)[..., None] * inkeys[:, :, None, None, :]
    readout_key_vector = jnp.einsum('sgrpn,sgn->sgrp', updated_state, readkeys, precision=lax.Precision.HIGHEST)
    readout_key_vector = readout_key_vector + skip_group[None, :, :, None] * values
    return (updated_state.reshape(layer_recurrent_state.shape), readout_key_vector.reshape(seq_count, heads_here * head_width))

def group_norm(gated_out, gain_layer, group_width):
    seq_count = gated_out.shape[0]
    grouped = gated_out.reshape(seq_count, -1, group_width)
    scaled = grouped * lax.rsqrt(lax.optimization_barrier(jnp.mean(grouped * grouped, axis=2, keepdims=True)) + EPSILON)
    return (scaled.reshape(seq_count, -1) * gain_layer[None]).astype(jnp.bfloat16)

def reference(residual_token_input, sequence_token_count, input_norm_gain, value_projection, input_key_projection, readout_key_projection, gate_projection, step_size_projection, convolution_weights, convolution_history, step_size_bias, head_decay_logarithm, direct_path_gain, extra_decay_logarithm, recurrent_state, output_norm_gain, output_projection):
    group_width = HEADS * HEAD_DIM // GROUPS
    hidden = residual_token_input
    states_new = []
    windows_new = []
    for layer_position in range(LAYERS):
        hidden_float = hidden.astype(jnp.float32)
        squares = lax.optimization_barrier(jnp.sum(hidden_float * hidden_float, axis=1))
        inverse = lax.rsqrt(squares / D + EPSILON)[:, None]
        scaled_in = (hidden_float * input_norm_gain[layer_position][None]).astype(jnp.bfloat16)

        def project_in(weight):
            return (inverse * jnp.dot(scaled_in, weight, preferred_element_type=jnp.float32)).astype(jnp.bfloat16)
        current = jnp.stack([project_in(value_projection[layer_position]), project_in(input_key_projection[layer_position]), project_in(readout_key_projection[layer_position])], axis=1)
        gate_in = project_in(gate_projection[layer_position])
        step_size_input = project_in(step_size_projection[layer_position])
        mixer_input_normed = conv_mixed(current, convolution_history[layer_position], convolution_weights[layer_position], sequence_token_count)
        windows_new.append(jnp.concatenate([convolution_history[layer_position][:, 1:], current[:, None]], axis=1))
        updated_state, readout_key_vector = state_after_update(recurrent_state[layer_position], extra_decay_logarithm[layer_position], mixer_input_normed, step_size_input, step_size_bias[layer_position], head_decay_logarithm[layer_position], direct_path_gain[layer_position])
        states_new.append(updated_state)
        gated_out = readout_key_vector * jax.nn.silu(gate_in.astype(jnp.float32))
        normed = group_norm(gated_out, output_norm_gain[layer_position], group_width)
        update = jnp.dot(normed, output_projection[layer_position], preferred_element_type=jnp.float32)
        hidden = (hidden_float + update).astype(jnp.bfloat16)
    return (hidden, jnp.stack(states_new), jnp.stack(windows_new))
```

```python
import functools

import jax
import jax.numpy as jnp
from jax import lax
from jax.experimental import pallas as pl
from jax.experimental.pallas import tpu as pltpu
from jax.sharding import PartitionSpec as P

D = 4096
EPSILON = 1e-06
MESH = pl.DeviceIdType.MESH
F32 = jnp.float32
BF16 = jnp.bfloat16
REACH = 4
STAT = 3


def total_wait(buffer, count, sem):
    part = buffer.at[pl.ds(0, count)]
    pltpu.make_async_copy(part, part, sem).wait()


def kernel(
    n_tp,
    n_dp,
    h_in,
    counts,
    in_gain,
    w_value,
    w_inkey,
    w_readkey,
    w_gate,
    w_step,
    taps,
    history,
    step_bias,
    decay_log,
    direct_gain,
    extra_log,
    state_in,
    out_gain,
    w_out,
    hidden_out,
    state_out,
    window_out,
    h_v,
    wp_v,
    ws_v,
    wo_v,
    hist_v,
    state_v,
    hist_f,
    early_v,
    cur_f,
    normed_f,
    tile_f,
    res_f,
    in_send,
    in_recv,
    mix_send,
    mix_recv,
    part_send,
    part_recv,
    own_send,
    own_recv,
    load_sem,
    state_sem,
    send_sem,
    recv_sem,
    far_sem,
):
    layers = w_out.shape[0]
    batch, feats = h_in.shape
    rows = batch // n_dp
    chans = w_out.shape[1]
    blocks = feats // 128
    head_dim = state_in.shape[3]
    heads = state_in.shape[2]
    width_back = history.shape[2]
    me_tp = lax.axis_index("tp")
    me_dp = lax.axis_index("dp")

    def tp_at(shift):
        return {"tp": lax.rem(me_tp + (n_tp + shift), n_tp)}

    def dp_at(shift):
        return {"dp": lax.rem(me_dp + shift, n_dp)}

    barrier = pltpu.get_barrier_semaphore()
    for shift in range(1, n_dp):
        pl.semaphore_signal(barrier, inc=1, device_id=dp_at(shift), device_id_type=MESH)
    for shift in range(1, REACH + 1):
        for to in (shift, -shift):
            pl.semaphore_signal(barrier, inc=1, device_id=tp_at(to), device_id_type=MESH)

    loads = [pltpu.make_async_copy(h_in, h_v, load_sem.at[0])]
    for l in range(layers):
        for k, w in enumerate((w_value, w_inkey, w_readkey, w_gate)):
            loads.append(pltpu.make_async_copy(w.at[l], wp_v.at[l, k], load_sem.at[1 + l]))
        loads.append(pltpu.make_async_copy(w_step.at[l], ws_v.at[l], load_sem.at[1 + l]))
        if l == 0:
            loads.append(pltpu.make_async_copy(history, hist_v, load_sem.at[3]))
            loads.append(pltpu.make_async_copy(state_in.at[0], state_v.at[0], load_sem.at[4]))
            loads.append(pltpu.make_async_copy(w_out.at[0], wo_v.at[0], load_sem.at[5]))
        else:
            loads.append(pltpu.make_async_copy(state_in.at[l], state_v.at[l], load_sem.at[6]))
            loads.append(pltpu.make_async_copy(w_out.at[l], wo_v.at[l], load_sem.at[7]))
    for load in loads:
        load.start()

    lane = lax.broadcasted_iota(jnp.int32, (rows, 128), 1)
    lane_all = lax.broadcasted_iota(jnp.int32, (batch, 128), 1)
    sub = lax.broadcasted_iota(jnp.int32, (rows, 128), 0)
    first_head = lane < head_dim

    def spread(values, in_layer):
        return jnp.where(first_head, values[in_layer, 0], values[in_layer, 1])

    def project(l, h):
        squares = jnp.sum(h * h, axis=1, keepdims=True)
        scaled = (h * in_gain[l : l + 1, :]).astype(BF16)
        for k in range(4):
            part = jnp.dot(scaled, wp_v[l, k], preferred_element_type=F32)
            for i in range(n_dp):
                in_send[l, i, k] = part[i * rows : (i + 1) * rows].astype(BF16)
        steps = jnp.dot(scaled, ws_v[l], preferred_element_type=F32)
        lane_step = lax.broadcasted_iota(jnp.int32, steps.shape, 1)
        wanted = [
            jnp.sum(jnp.where(lane_step == me_tp * heads + k, steps, 0.0), axis=1, keepdims=True)
            for k in range(heads)
        ] + [squares]
        stats = jnp.zeros((batch, 128), F32)
        for k, v in enumerate(wanted):
            high = v.astype(BF16).astype(F32)
            stats = jnp.where(lane_all == k, high, stats)
            stats = jnp.where(lane_all == k + STAT, v - high, stats)
        for i in range(n_dp):
            in_send[l, i, 4] = stats[i * rows : (i + 1) * rows].astype(BF16)
        in_recv[l, me_dp] = in_send[l, me_dp]

    def send_in(l):
        for shift in range(1, n_dp):
            to = dp_at(shift)
            pltpu.make_async_remote_copy(
                src_ref=in_send.at[l, to["dp"]],
                dst_ref=in_recv.at[l, me_dp],
                send_sem=send_sem.at[l],
                recv_sem=recv_sem.at[l],
                device_id=to,
                device_id_type=MESH,
            ).start()

    def earlier(l):
        lens = jnp.zeros((rows, 128), jnp.int32)
        for b in range(rows):
            lens = jnp.where(sub == b, counts[b], lens)
        for b in range(rows):
            for j in range(width_back):
                hist_f[pl.ds((b * width_back + j) * 4, 3), :] = hist_v[l, b, j].astype(F32)
        weights = taps[l].astype(F32)
        for r in range(3):
            total = jnp.zeros((rows, 128), F32)
            for j in range(width_back):
                past = hist_f[pl.ds(j * 4 + r, rows, stride=4 * width_back), :]
                live = jnp.where(lens >= width_back - j, past, 0.0)
                total = total + live * weights[j, r : r + 1]
            early_v[l, r] = total + 0.0
        for b in range(rows):
            for j in range(1, width_back):
                window_out[l, b, j - 1] = hist_v[l, b, j]

    def mixer(l):
        arrived = jnp.sum(in_recv[l].astype(F32), axis=0)
        stats = arrived[4]

        def stat(k):
            both = jnp.where((lane == k) | (lane == k + STAT), stats, 0.0)
            return jnp.sum(both, axis=1, keepdims=True)

        inverse = lax.rsqrt(stat(heads) / D + EPSILON)
        current = [(inverse * arrived[k]).astype(BF16).astype(F32) for k in range(3)]
        gate = (inverse * arrived[3]).astype(BF16).astype(F32)
        step = jnp.where(first_head, stat(0), stat(1)) * inverse
        step = step.astype(BF16).astype(F32)
        weights = taps[l].astype(F32)
        mixed = [
            jax.nn.silu(early_v[l, r] + current[r] * weights[width_back, r : r + 1])
            for r in range(3)
        ]
        value, inkey, readkey = mixed
        rate = jax.nn.softplus(step + spread(step_bias, l))
        extra = jnp.where(first_head, extra_log[l, :, 0:1], extra_log[l, :, 1:2])
        decay = jnp.exp(-rate * jnp.exp(spread(decay_log, l)) + extra)
        gain = rate * value
        gain_t = jnp.transpose(jnp.concatenate([gain] * (128 // rows), axis=0))
        lane_sq = lax.broadcasted_iota(jnp.int32, (head_dim, 128), 1)
        reads = [jnp.zeros((head_dim, 128), F32) for _ in range(heads)]
        for b in range(rows):
            key_b = jnp.broadcast_to(inkey[b : b + 1], (head_dim, 128))
            read_b = jnp.broadcast_to(readkey[b : b + 1], (head_dim, 128))
            for k in range(heads):
                decay_b = decay[b : b + 1, k * head_dim : k * head_dim + 1]
                column = gain_t[k * head_dim : (k + 1) * head_dim, b : b + 1]
                new = decay_b * state_v[l, b, k] + column * key_b
                state_v[l, b, k] = new
                read = jnp.sum(new * read_b, axis=1, keepdims=True)
                reads[k] = jnp.where(lane_sq == b, read, reads[k])
        pltpu.make_async_copy(state_v.at[l], state_out.at[l], state_sem).start()
        readout = jnp.transpose(jnp.concatenate(reads, axis=0))[0:rows]
        readout = readout + spread(direct_gain, l) * value
        gated = readout * jax.nn.silu(gate)
        scale = lax.rsqrt(jnp.mean(gated * gated, axis=1, keepdims=True) + EPSILON)
        normed = (gated * scale * out_gain[l : l + 1, :]).astype(BF16)
        mix_send[l] = normed
        mix_recv[l, me_dp] = normed
        for r in range(3):
            cur_f[pl.ds(r, rows, stride=4), :] = current[r]
        for b in range(rows):
            window_out[l, b, width_back - 1] = cur_f[pl.ds(4 * b, 3), :].astype(BF16)

    def send_mix(l):
        for shift in range(1, n_dp):
            pltpu.make_async_remote_copy(
                src_ref=mix_send.at[l],
                dst_ref=mix_recv.at[l, me_dp],
                send_sem=send_sem.at[layers + l],
                recv_sem=recv_sem.at[layers + l],
                device_id=dp_at(shift),
                device_id_type=MESH,
            ).start()

    def ring_send(source, target, sem):
        def pair(step, _):
            shift = n_tp // 2 - step

            def to(shift):
                at = lax.rem(me_tp + shift, n_tp)
                pltpu.make_async_remote_copy(
                    src_ref=source(at),
                    dst_ref=target,
                    send_sem=send_sem.at[sem],
                    recv_sem=recv_sem.at[sem],
                    device_id={"tp": at},
                    device_id_type=MESH,
                ).start()

            to(shift)
            to(n_tp - shift)
            return 0

        at_far = lax.rem(me_tp + n_tp // 2, n_tp)
        pltpu.make_async_remote_copy(
            src_ref=source(at_far),
            dst_ref=target,
            send_sem=send_sem.at[sem],
            recv_sem=recv_sem.at[sem],
            device_id={"tp": at_far},
            device_id_type=MESH,
        ).start()
        lax.fori_loop(1, n_tp // 2, pair, 0)

    loads[0].wait()
    h = h_v[...].astype(F32)
    for i in range(n_dp):
        for j in range(blocks):
            res_f[i * blocks + j] = h[i * rows : (i + 1) * rows, j * 128 : (j + 1) * 128]
    for load in loads[1:6]:
        load.wait()
    project(0, h)
    pl.semaphore_wait(barrier, n_dp - 1 + 2 * REACH)
    for to in (REACH, -REACH):
        pl.semaphore_signal(far_sem.at[0], inc=1, device_id=tp_at(to), device_id_type=MESH)
    send_in(0)
    loads[6].wait()
    earlier(0)
    earlier(1)
    loads[7].wait()

    for l in range(layers):
        total_wait(in_recv.at[l], n_dp - 1, recv_sem.at[l])
        mixer(l)
        if l == 0:
            pl.semaphore_wait(far_sem.at[0], 2)
            for to in (2 * REACH, -2 * REACH):
                pl.semaphore_signal(
                    far_sem.at[1], inc=1, device_id=tp_at(to), device_id_type=MESH
                )
        send_mix(l)
        loads[8 if l == 0 else 15].wait()
        total_wait(mix_recv.at[l], n_dp - 1, recv_sem.at[layers + l])
        if l + 1 < layers:
            mix = jnp.concatenate(
                [mix_recv[l, i].astype(F32) for i in range(n_dp)], axis=0
            ).astype(BF16)
            part = jnp.dot(mix, wo_v[l], preferred_element_type=F32)
            for i in range(n_dp):
                for j in range(blocks):
                    part_send[l, i * blocks + j] = part[
                        i * rows : (i + 1) * rows, j * 128 : (j + 1) * 128
                    ].astype(BF16)
            part_recv[l, me_tp] = part_send[l, me_tp]
            pl.semaphore_wait(far_sem.at[1], 2)
            ring_send(lambda at: part_send.at[l, at], part_recv.at[l, me_tp], 2 * layers + l)
            total_wait(part_recv.at[l], n_tp - 1, recv_sem.at[2 * layers + l])
            mine = jnp.sum(part_recv[l].astype(F32), axis=0) + res_f[me_tp]
            own_send[...] = mine.astype(BF16)
            own_recv[me_tp] = mine.astype(BF16)
            ring_send(lambda at: own_send, own_recv.at[me_tp], 3 * layers)
            for load in loads[9:15]:
                load.wait()
            total_wait(own_recv, n_tp - 1, recv_sem.at[3 * layers])
            h = jnp.concatenate(
                [
                    jnp.concatenate(
                        [own_recv[i * blocks + j].astype(F32) for j in range(blocks)], axis=1
                    )
                    for i in range(n_dp)
                ],
                axis=0,
            )
            project(l + 1, h)
            send_in(l + 1)
            h_v[...] = h.astype(BF16)
        else:
            for i in range(n_dp):
                normed_f[i * rows : (i + 1) * rows, :] = mix_recv[l, i].astype(F32)
            mix = jnp.concatenate(
                [normed_f[pl.ds(r, batch // 2, stride=2), :] for r in range(2)], axis=0
            ).astype(BF16)
            part = jnp.dot(mix, wo_v[l], preferred_element_type=F32)
            for j in range(blocks):
                for r in range(2):
                    tile_f[pl.ds(2 * j + r, n_tp, stride=8), :] = part[
                        r * n_tp : (r + 1) * n_tp, j * 128 : (j + 1) * 128
                    ]
            for i in range(n_tp):
                part_send[l, i] = tile_f[i * 8 : (i + 1) * 8, :].astype(BF16)
            part_recv[l, me_tp] = part_send[l, me_tp]
            ring_send(lambda at: part_send.at[l, at], part_recv.at[l, me_tp], 2 * layers + l)
            at_row = lax.broadcasted_iota(jnp.int32, (8, batch), 0)
            at_col = lax.broadcasted_iota(jnp.int32, (8, batch), 1)
            pick = ((at_col == 2 * me_tp + at_row) & (at_row < 2)).astype(BF16)
            kept = jnp.dot(pick, h_v[...], preferred_element_type=F32)[0:2]
            total_wait(part_recv.at[l], n_tp - 1, recv_sem.at[2 * layers + l])
            tile = jnp.sum(part_recv[l].astype(F32), axis=0)
            update = jnp.concatenate([tile[2 * j : 2 * j + 2] for j in range(blocks)], axis=1)
            hidden_out[...] = (kept + update).astype(BF16)

    for l in range(layers):
        total_wait(in_send.at[l], n_dp - 1, send_sem.at[l])
        for _ in range(n_dp - 1):
            pltpu.make_async_copy(mix_send.at[l], mix_send.at[l], send_sem.at[layers + l]).wait()
        total_wait(part_send.at[l], n_tp - 1, send_sem.at[2 * layers + l])
        pltpu.make_async_copy(state_v.at[l], state_out.at[l], state_sem).wait()
    total_wait(own_recv, n_tp - 1, send_sem.at[3 * layers])


def body(n_tp, n_dp, *args):
    h, _, _, w_value = args[:4]
    w_step, history, state, w_out = args[7], args[9], args[14], args[16]
    layers, feats, chans = w_value.shape
    batch = h.shape[0]
    rows = batch // n_dp
    vmem = pl.BlockSpec(memory_space=pltpu.VMEM)
    smem = pl.BlockSpec(memory_space=pltpu.SMEM)
    hbm = pl.BlockSpec(memory_space=pl.ANY)
    in_specs = [
        hbm, smem, vmem, hbm, hbm, hbm, hbm, hbm, vmem, hbm, smem, smem, smem, vmem, hbm, vmem, hbm,
    ]
    return pl.pallas_call(
        functools.partial(kernel, n_tp, n_dp),
        out_shape=(
            jax.ShapeDtypeStruct((batch // n_tp, feats), BF16),
            jax.ShapeDtypeStruct(state.shape, F32),
            jax.ShapeDtypeStruct(history.shape, BF16),
        ),
        in_specs=in_specs,
        out_specs=(vmem, hbm, vmem),
        scratch_shapes=[
            pltpu.VMEM((batch, feats), BF16),
            pltpu.VMEM((layers, 4, feats, chans), BF16),
            pltpu.VMEM(w_step.shape, BF16),
            pltpu.VMEM(w_out.shape, BF16),
            pltpu.VMEM(history.shape, BF16),
            pltpu.VMEM(state.shape, F32),
            pltpu.VMEM((rows * 16, 128), F32),
            pltpu.VMEM((layers, 3, rows, 128), F32),
            pltpu.VMEM((rows * 4, 128), F32),
            pltpu.VMEM((batch, 128), F32),
            pltpu.VMEM((n_tp * 8, 128), F32),
            pltpu.VMEM((n_tp, 8, 128), F32),
            pltpu.VMEM((layers, n_dp, 5, rows, 128), BF16),
            pltpu.VMEM((layers, n_dp, 5, rows, 128), BF16),
            pltpu.VMEM((layers, rows, 128), BF16),
            pltpu.VMEM((layers, n_dp, rows, 128), BF16),
            pltpu.VMEM((layers, n_tp, 8, 128), BF16),
            pltpu.VMEM((layers, n_tp, 8, 128), BF16),
            pltpu.VMEM((8, 128), BF16),
            pltpu.VMEM((n_tp, 8, 128), BF16),
            pltpu.SemaphoreType.DMA((8,)),
            pltpu.SemaphoreType.DMA,
            pltpu.SemaphoreType.DMA((3 * layers + 1,)),
            pltpu.SemaphoreType.DMA((3 * layers + 1,)),
            pltpu.SemaphoreType.REGULAR((2,)),
        ],
        compiler_params=pltpu.CompilerParams(collective_id=0, has_side_effects=True),
    )(*args)


def solution(mesh):
    placed = (
        P("grp", "dp"),
        P(("grp", "dp")),
        P(None, "dp"),
        P(None, "dp", "tp"),
        P(None, "dp", "tp"),
        P(None, "dp", "tp"),
        P(None, "dp", "tp"),
        P(None, "dp", None),
        P(None, None, None, "tp"),
        P(None, ("grp", "dp"), None, None, "tp"),
        P(None, "tp"),
        P(None, "tp"),
        P(None, "tp"),
        P(None, ("grp", "dp"), "tp"),
        P(None, ("grp", "dp"), "tp", None, None),
        P(None, "tp"),
        P(None, "tp", "dp"),
    )
    return jax.shard_map(
        functools.partial(body, mesh.shape["tp"], mesh.shape["dp"]),
        mesh=mesh,
        in_specs=placed,
        out_specs=(
            P(("grp", "tp"), "dp"),
            P(None, ("grp", "dp"), "tp", None, None),
            P(None, ("grp", "dp"), None, None, "tp"),
        ),
        check_vma=False,
    )
```

```python
import functools

import jax
import jax.numpy as jnp
from jax import lax
from jax.experimental import pallas as pl
from jax.experimental.pallas import tpu as pltpu
from jax.sharding import PartitionSpec as P

D = 4096
EPSILON = 1e-06
MESH = pl.DeviceIdType.MESH
F32 = jnp.float32
BF16 = jnp.bfloat16
LANES = 128
STAT = 3


def total_wait(buffer, count, sem):
    part = buffer.at[pl.ds(0, count)]
    pltpu.make_async_copy(part, part, sem).wait()


def kernel(
    n_tp,
    n_dp,
    h_in,
    counts,
    in_gain,
    w_value,
    w_inkey,
    w_readkey,
    w_gate,
    w_step,
    taps,
    history,
    step_bias,
    decay_log,
    direct_gain,
    extra_log,
    state_in,
    out_gain,
    w_out,
    hidden_out,
    state_out,
    window_out,
    h_v,
    wp_v,
    wo_v,
    hist_v,
    state_v,
    hist_f,
    win_f,
    early_v,
    normed_f,
    tile_f,
    in_send,
    in_recv,
    mix_send,
    mix_recv,
    near_send,
    near_recv,
    far_recv,
    own_recv,
    part_send,
    part_recv,
    load_sem,
    state_sem,
    send_sem,
    recv_sem,
    know_sem,
):
    layers = w_out.shape[0]
    batch, feats = h_in.shape
    rows = batch // n_dp
    blocks = feats // LANES
    head_dim = state_in.shape[3]
    heads = state_in.shape[2]
    roles, width_back = history.shape[2:4]
    far = n_tp // blocks
    me_tp = lax.axis_index("tp")
    me_dp = lax.axis_index("dp")
    me_block = me_tp // blocks
    me_quarter = lax.rem(me_tp, blocks)

    def tp_at(shift):
        return {"tp": lax.rem(me_tp + (n_tp + shift), n_tp)}

    def dp_at(shift):
        return {"dp": lax.rem(me_dp + shift, n_dp)}

    def near_at(shift):
        return {"tp": me_block * blocks + lax.rem(me_quarter + shift, blocks)}

    def remote(source, target, sem, to):
        pltpu.make_async_remote_copy(
            src_ref=source,
            dst_ref=target,
            send_sem=send_sem.at[sem],
            recv_sem=recv_sem.at[sem],
            device_id=to,
            device_id_type=MESH,
        ).start()

    def signal(sem, to):
        pl.semaphore_signal(sem, inc=1, device_id=to, device_id_type=MESH)

    in_at = lambda l: l
    mix_at = lambda l: layers + l
    near_sum, far_sum, near_all, ring_sum = (2 * layers + k for k in range(4))

    barrier = pltpu.get_barrier_semaphore()
    for shift in range(1, n_dp):
        signal(barrier, dp_at(shift))
    for shift in range(1, blocks + 1):
        for to in (shift, -shift):
            signal(barrier, tp_at(to))

    def load(source, target, sem):
        copy = pltpu.make_async_copy(source, target, load_sem.at[sem])
        copy.start()
        return copy

    h_load = load(h_in, h_v, 0)
    w_loads, state_loads, wo_loads = [], [], []
    for l in range(layers):
        w_loads.append(
            [
                load(w.at[l], wp_v.at[l, :, pl.ds(k * LANES, LANES)], 1 + l)
                for k, w in enumerate((w_value, w_inkey, w_readkey, w_gate))
            ]
        )
        if l == 0:
            hist_load = load(history, hist_v, 1 + layers)
        state_loads.append(load(state_in.at[l], state_v.at[l], 2 + layers + l))
        wo_loads.append(load(w_out.at[l], wo_v.at[l], 2 + 2 * layers + l))

    lane = lax.broadcasted_iota(jnp.int32, (rows, LANES), 1)
    lane_all = lax.broadcasted_iota(jnp.int32, (batch, LANES), 1)
    sub = lax.broadcasted_iota(jnp.int32, (rows, LANES), 0)
    first_head = lane < head_dim

    def spread(values, in_layer):
        return jnp.where(first_head, values[in_layer, 0], values[in_layer, 1])

    def project(l, h):
        with jax.named_scope(f"proj{l}"):
            squares = jnp.sum(h * h, axis=1, keepdims=True)
            scaled = (h * in_gain[l : l + 1, :]).astype(BF16)
            steps = lax.dot_general(
                scaled, w_step[l], (((1,), (1,)), ((), ())), preferred_element_type=F32
            )
            lane_step = lax.broadcasted_iota(jnp.int32, steps.shape, 1)
            wanted = [
                jnp.sum(
                    jnp.where(lane_step == me_tp * heads + k, steps, 0.0), axis=1, keepdims=True
                )
                for k in range(heads)
            ] + [squares]
            for load in w_loads[l]:
                load.wait()
            part = jnp.dot(scaled, wp_v[l], preferred_element_type=F32)
            stats = jnp.zeros((batch, LANES), F32)
            for k, v in enumerate(wanted):
                high = v.astype(BF16).astype(F32)
                stats = jnp.where(lane_all == k, high, stats)
                stats = jnp.where(lane_all == k + STAT, v - high, stats)
            for i in range(n_dp):
                at = slice(i * rows, (i + 1) * rows)
                for k in range(4):
                    in_send[l, i, k] = part[at, k * LANES : (k + 1) * LANES].astype(BF16)
                in_send[l, i, 4] = stats[at].astype(BF16)

    def send_in(l):
        for shift in range(1, n_dp):
            to = dp_at(shift)
            remote(in_send.at[l, to["dp"]], in_recv.at[l, me_dp], in_at(l), to)
        in_recv[l, me_dp] = in_send[l, me_dp]

    def earlier(l):
        lens = jnp.zeros((rows, LANES), jnp.int32)
        for b in range(rows):
            lens = jnp.where(sub == b, counts[b], lens)
        for b in range(rows):
            for r in range(roles):
                hist_f[pl.ds((b * roles + r) * width_back, width_back), :] = hist_v[
                    l, b, r
                ].astype(F32)
        for r in range(roles):
            total = jnp.zeros((rows, LANES), F32)
            for j in range(width_back):
                past = hist_f[pl.ds(r * width_back + j, rows, stride=roles * width_back), :]
                live = jnp.where(lens >= width_back - j, past, 0.0)
                total = total + live * taps[j, r, l : l + 1].astype(F32)
                if j:
                    win_f[
                        l, pl.ds(r * width_back + j - 1, rows, stride=roles * width_back), :
                    ] = past
            early_v[l, r] = total

    def window(l):
        for b in range(rows):
            for r in range(roles):
                window_out[l, b, r] = win_f[
                    l, pl.ds((b * roles + r) * width_back, width_back), :
                ].astype(BF16)

    def mixer(l):
        with jax.named_scope(f"mixer{l}"):
            arrived = jnp.sum(in_recv[l].astype(F32), axis=0)
            stats = arrived[4]

            def stat(k):
                both = jnp.where((lane == k) | (lane == k + STAT), stats, 0.0)
                return jnp.sum(both, axis=1, keepdims=True)

            inverse = lax.rsqrt(stat(heads) / D + EPSILON)
            current = [(inverse * arrived[k]).astype(BF16).astype(F32) for k in range(roles)]
            gate = (inverse * arrived[3]).astype(BF16).astype(F32)
            step = jnp.where(first_head, stat(0), stat(1)) * inverse
            step = step.astype(BF16).astype(F32)
            value, inkey, readkey = [
                jax.nn.silu(
                    early_v[l, r] + current[r] * taps[width_back, r, l : l + 1].astype(F32)
                )
                for r in range(roles)
            ]
            rate = jax.nn.softplus(step + spread(step_bias, l))
            diagonal = lax.broadcasted_iota(
                jnp.int32, (rows, rows), 0
            ) == lax.broadcasted_iota(jnp.int32, (rows, rows), 1)
            extra = [
                jnp.sum(
                    jnp.where(diagonal, extra_log[l, k : k + 1, :], 0.0), axis=1, keepdims=True
                )
                for k in range(heads)
            ]
            extra = jnp.where(first_head, extra[0], extra[1])
            decay = jnp.exp(-rate * jnp.exp(spread(decay_log, l)) + extra)
            gain = rate * value
            gain_t = jnp.transpose(jnp.concatenate([gain] * (LANES // rows), axis=0))
            lane_sq = lax.broadcasted_iota(jnp.int32, (head_dim, LANES), 1)
            reads = [jnp.zeros((head_dim, LANES), F32) for _ in range(heads)]
            for b in range(rows):
                key_b = jnp.broadcast_to(inkey[b : b + 1], (head_dim, LANES))
                read_b = jnp.broadcast_to(readkey[b : b + 1], (head_dim, LANES))
                for k in range(heads):
                    decay_b = decay[b : b + 1, k * head_dim : k * head_dim + 1]
                    column = gain_t[k * head_dim : (k + 1) * head_dim, b : b + 1]
                    new = decay_b * state_v[l, b, k] + column * key_b
                    state_v[l, b, k] = new
                    read = jnp.sum(new * read_b, axis=1, keepdims=True)
                    reads[k] = jnp.where(lane_sq == b, read, reads[k])
            readout = jnp.transpose(jnp.concatenate(reads, axis=0))[0:rows]
            readout = readout + spread(direct_gain, l) * value
            gated = readout * jax.nn.silu(gate)
            scale = lax.rsqrt(jnp.mean(gated * gated, axis=1, keepdims=True) + EPSILON)
            normed = (gated * scale * out_gain[l : l + 1, :]).astype(BF16)
            mix_send[l] = normed
            mix_recv[l, me_dp] = normed
            for r in range(roles):
                win_f[
                    l, pl.ds((r + 1) * width_back - 1, rows, stride=roles * width_back), :
                ] = current[r]

    def send_mix(l):
        for shift in range(1, n_dp):
            remote(mix_send.at[l], mix_recv.at[l, me_dp], mix_at(l), dp_at(shift))
        pltpu.make_async_copy(state_v.at[l], state_out.at[l], state_sem).start()

    def reduce_all(l):
        with jax.named_scope("near_sum"):
            mix = jnp.concatenate(
                [mix_recv[l, i].astype(F32) for i in range(n_dp)], axis=0
            ).astype(BF16)
            part = jnp.dot(mix, wo_v[l], preferred_element_type=F32)
            for j in range(blocks):
                near_send[j] = part[:, j * LANES : (j + 1) * LANES].astype(BF16)
            for shift in range(1, blocks):
                to = near_at(shift)
                quarter = lax.rem(me_quarter + shift, blocks)
                remote(near_send.at[quarter], near_recv.at[me_quarter], near_sum, to)
            near_recv[me_quarter] = near_send[me_quarter]
            h = h_v[:, pl.ds(pl.multiple_of(me_quarter * LANES, LANES), LANES)].astype(F32)
        with jax.named_scope("near_wait"):
            total_wait(near_recv, blocks - 1, recv_sem.at[near_sum])
        with jax.named_scope("far_send"):
            far_recv[me_block] = jnp.sum(near_recv[...].astype(F32), axis=0).astype(BF16)
            pl.semaphore_wait(know_sem.at[1], 2)
            for step in range(far // 2, 0, -1):
                for shift in sorted({step, far - step}):
                    to = tp_at(shift * blocks)
                    remote(far_recv.at[me_block], far_recv.at[me_block], far_sum, to)
        with jax.named_scope("far_wait"):
            for load in w_loads[l + 1]:
                pass
            total_wait(far_recv, far - 1, recv_sem.at[far_sum])
        with jax.named_scope("near_all"):
            mine = (h + jnp.sum(far_recv[...].astype(F32), axis=0)).astype(BF16)
            own_recv[me_quarter] = mine
            for shift in range(1, blocks):
                remote(own_recv.at[me_quarter], own_recv.at[me_quarter], near_all, near_at(shift))
        with jax.named_scope("near_all_wait"):
            total_wait(own_recv, blocks - 1, recv_sem.at[near_all])
        return jnp.concatenate([own_recv[j].astype(F32) for j in range(blocks)], axis=1)

    def reduce_rows(l):
        with jax.named_scope("ring_send"):
            for i in range(n_dp):
                normed_f[i * rows : (i + 1) * rows, :] = mix_recv[l, i].astype(F32)
            kept_rows = batch // n_tp
            mix = jnp.concatenate(
                [normed_f[pl.ds(r, n_tp, stride=kept_rows), :] for r in range(kept_rows)], axis=0
            ).astype(BF16)
            part = jnp.dot(mix, wo_v[l], preferred_element_type=F32)
            for j in range(blocks):
                for r in range(kept_rows):
                    tile_f[pl.ds(kept_rows * j + r, n_tp, stride=8), :] = part[
                        r * n_tp : (r + 1) * n_tp, j * LANES : (j + 1) * LANES
                    ]
            for i in range(n_tp):
                part_send[i] = tile_f[i * 8 : (i + 1) * 8, :].astype(BF16)

            def to(shift):
                at = lax.rem(me_tp + shift, n_tp)
                remote(part_send.at[at], part_recv.at[me_tp], ring_sum, {"tp": at})

            def pair(step, _):
                to(n_tp // 2 - step)
                to(n_tp // 2 + step)
                return 0

            to(n_tp // 2)
            lax.fori_loop(1, n_tp // 2, pair, 0)
            part_recv[me_tp] = part_send[me_tp]
        with jax.named_scope("ring_wait"):
            at_row = lax.broadcasted_iota(jnp.int32, (8, batch), 0)
            at_col = lax.broadcasted_iota(jnp.int32, (8, batch), 1)
            pick = ((at_col == kept_rows * me_tp + at_row) & (at_row < kept_rows)).astype(BF16)
            h = jnp.concatenate([own_recv[j] for j in range(blocks)], axis=1)
            kept = jnp.dot(pick, h, preferred_element_type=F32)[0:kept_rows]
            window(l)
            total_wait(part_recv, n_tp - 1, recv_sem.at[ring_sum])
        with jax.named_scope("ring_sum"):
            tile = jnp.sum(part_recv[...].astype(F32), axis=0)
            update = jnp.concatenate(
                [tile[kept_rows * j : kept_rows * (j + 1)] for j in range(blocks)], axis=1
            )
            hidden_out[...] = (kept + update).astype(BF16)

    h_load.wait()
    project(0, h_v[...].astype(F32))
    with jax.named_scope("barrier"):
        pl.semaphore_wait(barrier, n_dp - 1 + 2 * blocks)
    for to in (blocks, -blocks):
        signal(know_sem.at[0], tp_at(to))
    with jax.named_scope("send_in0"):
        send_in(0)
        hist_load.wait()
        for l in range(layers):
            earlier(l)
        state_loads[0].wait()

    for l in range(layers):
        with jax.named_scope(f"in_wait{l}"):
            total_wait(in_recv.at[l], n_dp - 1, recv_sem.at[in_at(l)])
        mixer(l)
        if l == 0:
            pl.semaphore_wait(know_sem.at[0], 2)
            for to in (2 * blocks, -2 * blocks):
                signal(know_sem.at[1], tp_at(to))
        with jax.named_scope(f"mix_wait{l}"):
            send_mix(l)
            wo_loads[l].wait()
            if l == 0:
                window(l)
            total_wait(mix_recv.at[l], n_dp - 1, recv_sem.at[mix_at(l)])
        if l + 1 < layers:
            project(l + 1, reduce_all(l))
            with jax.named_scope(f"send_in{l + 1}"):
                send_in(l + 1)
                state_loads[l + 1].wait()
        else:
            reduce_rows(l)

    with jax.named_scope("end"):
        for l in range(layers):
            total_wait(in_send.at[l], n_dp - 1, send_sem.at[in_at(l)])
            total_wait(mix_recv.at[l], n_dp - 1, send_sem.at[mix_at(l)])
            pltpu.make_async_copy(state_v.at[l], state_out.at[l], state_sem).wait()
        total_wait(near_recv, blocks - 1, send_sem.at[near_sum])
        total_wait(far_recv, far - 1, send_sem.at[far_sum])
        total_wait(own_recv, blocks - 1, send_sem.at[near_all])
        total_wait(part_send, n_tp - 1, send_sem.at[ring_sum])


def body(n_tp, n_dp, *args):
    args = list(args)
    args[7] = jnp.transpose(args[7], (0, 2, 1))
    args[8] = jnp.transpose(args[8], (1, 2, 0, 3))
    args[9] = jnp.transpose(args[9], (0, 1, 3, 2, 4))
    args[13] = jnp.transpose(args[13], (0, 2, 1))
    h, w_value, history, state, w_out = (args[k] for k in (0, 3, 9, 14, 16))
    layers, feats, chans = w_value.shape
    batch = h.shape[0]
    rows = batch // n_dp
    roles, width_back = history.shape[2:4]
    blocks = feats // LANES
    vmem = pl.BlockSpec(memory_space=pltpu.VMEM)
    smem = pl.BlockSpec(memory_space=pltpu.SMEM)
    hbm = pl.BlockSpec(memory_space=pl.ANY)
    in_specs = [
        hbm, smem, vmem, hbm, hbm, hbm, hbm, vmem, vmem, hbm, smem, smem, smem, vmem, hbm, vmem, hbm,
    ]
    hidden, states, windows = pl.pallas_call(
        functools.partial(kernel, n_tp, n_dp),
        out_shape=(
            jax.ShapeDtypeStruct((batch // n_tp, feats), BF16),
            jax.ShapeDtypeStruct(state.shape, F32),
            jax.ShapeDtypeStruct(history.shape, BF16),
        ),
        in_specs=in_specs,
        out_specs=(vmem, hbm, vmem),
        scratch_shapes=[
            pltpu.VMEM((batch, feats), BF16),
            pltpu.VMEM((layers, feats, 4 * chans), BF16),
            pltpu.VMEM(w_out.shape, BF16),
            pltpu.VMEM(history.shape, BF16),
            pltpu.VMEM(state.shape, F32),
            pltpu.VMEM((rows * roles * width_back, LANES), F32),
            pltpu.VMEM((layers, rows * roles * width_back, LANES), F32),
            pltpu.VMEM((layers, roles, rows, LANES), F32),
            pltpu.VMEM((batch, LANES), F32),
            pltpu.VMEM((n_tp * 8, LANES), F32),
            pltpu.VMEM((layers, n_dp, 5, rows, LANES), BF16),
            pltpu.VMEM((layers, n_dp, 5, rows, LANES), BF16),
            pltpu.VMEM((layers, rows, LANES), BF16),
            pltpu.VMEM((layers, n_dp, rows, LANES), BF16),
            pltpu.VMEM((blocks, batch, LANES), BF16),
            pltpu.VMEM((blocks, batch, LANES), BF16),
            pltpu.VMEM((n_tp // blocks, batch, LANES), BF16),
            pltpu.VMEM((blocks, batch, LANES), BF16),
            pltpu.VMEM((n_tp, 8, LANES), BF16),
            pltpu.VMEM((n_tp, 8, LANES), BF16),
            pltpu.SemaphoreType.DMA((2 + 3 * layers,)),
            pltpu.SemaphoreType.DMA,
            pltpu.SemaphoreType.DMA((2 * layers + 4,)),
            pltpu.SemaphoreType.DMA((2 * layers + 4,)),
            pltpu.SemaphoreType.REGULAR((2,)),
        ],
        compiler_params=pltpu.CompilerParams(collective_id=0, has_side_effects=True),
    )(*args)
    return hidden, states, jnp.transpose(windows, (0, 1, 3, 2, 4))


def solution(mesh):
    placed = (
        P("grp", "dp"),
        P(("grp", "dp")),
        P(None, "dp"),
        P(None, "dp", "tp"),
        P(None, "dp", "tp"),
        P(None, "dp", "tp"),
        P(None, "dp", "tp"),
        P(None, "dp", None),
        P(None, None, None, "tp"),
        P(None, ("grp", "dp"), None, None, "tp"),
        P(None, "tp"),
        P(None, "tp"),
        P(None, "tp"),
        P(None, ("grp", "dp"), "tp"),
        P(None, ("grp", "dp"), "tp", None, None),
        P(None, "tp"),
        P(None, "tp", "dp"),
    )
    return jax.shard_map(
        functools.partial(body, mesh.shape["tp"], mesh.shape["dp"]),
        mesh=mesh,
        in_specs=placed,
        out_specs=(
            P(("grp", "tp"), "dp"),
            P(None, ("grp", "dp"), "tp", None, None),
            P(None, ("grp", "dp"), None, None, "tp"),
        ),
        check_vma=False,
    )
```

```python
import functools

import jax
import jax.numpy as jnp
from jax import lax
from jax.experimental import pallas as pl
from jax.experimental.pallas import tpu as pltpu
from jax.sharding import PartitionSpec as P

D = 4096
EPSILON = 1e-06
MESH = pl.DeviceIdType.MESH
F32 = jnp.float32
BF16 = jnp.bfloat16
LANES = 128
STAT = 3


def total_wait(buffer, count, sem):
    part = buffer.at[pl.ds(0, count)]
    pltpu.make_async_copy(part, part, sem).wait()


def kernel(
    n_tp,
    n_dp,
    h_in,
    counts_in,
    in_gain_in,
    w_value,
    w_inkey,
    w_readkey,
    w_gate,
    w_step_in,
    taps_in,
    history,
    step_bias_in,
    decay_log_in,
    direct_gain_in,
    extra_log_in,
    state_in,
    out_gain_in,
    w_out,
    hidden_out,
    state_out,
    window_out,
    counts,
    in_gain,
    w_step,
    taps,
    step_bias,
    decay_log,
    direct_gain,
    extra_log,
    out_gain,
    h_v,
    wp_v,
    wo_v,
    hist_v,
    state_v,
    hist_f,
    win_f,
    early_v,
    fixed_v,
    tile_f,
    in_send,
    in_recv,
    mix_recv,
    wide_recv,
    wo_near,
    far_recv,
    own_recv,
    part_send,
    part_recv,
    load_sem,
    send_sem,
    recv_sem,
    know_sem,
):
    layers = w_out.shape[0]
    batch, feats = h_in.shape
    rows = batch // n_dp
    blocks = feats // LANES
    head_dim = state_in.shape[3]
    heads = state_in.shape[2]
    roles, width_back = history.shape[2:4]
    far = n_tp // blocks
    me_tp = lax.axis_index("tp")
    me_dp = lax.axis_index("dp")
    me_block = me_tp // blocks
    me_quarter = lax.rem(me_tp, blocks)

    def tp_at(shift):
        return {"tp": lax.rem(me_tp + (n_tp + shift), n_tp)}

    def dp_at(shift):
        return {"dp": lax.rem(me_dp + shift, n_dp)}

    def near_at(shift):
        return {"tp": me_block * blocks + lax.rem(me_quarter + shift, blocks)}

    def remote(source, target, sem, to):
        pltpu.make_async_remote_copy(
            src_ref=source,
            dst_ref=target,
            send_sem=send_sem.at[sem],
            recv_sem=recv_sem.at[sem],
            device_id=to,
            device_id_type=MESH,
        ).start()

    def signal(sem, to):
        pl.semaphore_signal(sem, inc=1, device_id=to, device_id_type=MESH)

    in_at = lambda l: l
    mix_at = lambda l: layers + l
    weights_near, far_sum, near_all, ring_sum = (2 * layers + k for k in range(4))
    dp_shifts = sorted(range(1, n_dp), key=lambda s: abs(s - n_dp // 2))

    def load(source, target, sem):
        copy = pltpu.make_async_copy(source, target, load_sem.at[sem])
        copy.start()
        return copy

    h_load = [load(h_in, h_v, 0), load(in_gain_in, in_gain, 0)]
    w_loads, state_loads, wo_loads = [], [], []
    for l in range(layers):
        w_loads.append(
            [
                load(w.at[l], wp_v.at[l, :, pl.ds(k * LANES, LANES)], 1 + l)
                for k, w in enumerate((w_value, w_inkey, w_readkey, w_gate))
            ]
        )
        if l == 0:
            step_load = load(w_step_in, w_step, 1 + layers)
            small_loads = [
                load(source, target, 2 + layers)
                for source, target in (
                    (history, hist_v),
                    (counts_in, counts),
                    (taps_in, taps),
                    (step_bias_in, step_bias),
                    (decay_log_in, decay_log),
                    (direct_gain_in, direct_gain),
                    (extra_log_in, extra_log),
                    (out_gain_in, out_gain),
                )
            ]
        state_loads.append(load(state_in.at[l], state_v.at[l], 3 + layers + l))
        wo_loads.append(load(w_out.at[l], wo_v.at[l], 3 + 2 * layers + l))

    barrier = pltpu.get_barrier_semaphore()
    for shift in range(1, n_dp):
        signal(barrier, dp_at(shift))
    for shift in range(1, blocks + 1):
        for to in (shift, -shift):
            signal(barrier, tp_at(to))

    lane = lax.broadcasted_iota(jnp.int32, (rows, LANES), 1)
    lane_all = lax.broadcasted_iota(jnp.int32, (batch, LANES), 1)
    sub = lax.broadcasted_iota(jnp.int32, (rows, LANES), 0)
    first_head = lane < head_dim

    def spread(values, in_layer):
        return jnp.where(first_head, values[in_layer, 0], values[in_layer, 1])

    def project(l, h):
        with jax.named_scope(f"proj{l}"):
            squares = jnp.sum(h * h, axis=1, keepdims=True)
            scaled = (h * in_gain[l : l + 1, :]).astype(BF16)
            if l == 0:
                step_load.wait()
            steps = lax.dot_general(
                scaled, w_step[l], (((1,), (1,)), ((), ())), preferred_element_type=F32
            )
            lane_step = lax.broadcasted_iota(jnp.int32, steps.shape, 1)
            wanted = [
                jnp.sum(
                    jnp.where(lane_step == me_tp * heads + k, steps, 0.0), axis=1, keepdims=True
                )
                for k in range(heads)
            ] + [squares]
            if l == 0:
                for copy in w_loads[l]:
                    copy.wait()
            part = jnp.dot(scaled, wp_v[l], preferred_element_type=F32)
            stats = jnp.zeros((batch, LANES), F32)
            for k, v in enumerate(wanted):
                high = v.astype(BF16).astype(F32)
                stats = jnp.where(lane_all == k, high, stats)
                stats = jnp.where(lane_all == k + STAT, v - high, stats)
            for i in range(n_dp):
                at = slice(i * rows, (i + 1) * rows)
                for k in range(4):
                    in_send[l, i, k] = part[at, k * LANES : (k + 1) * LANES].astype(BF16)
                in_send[l, i, 4] = stats[at].astype(BF16)

    def send_in(l):
        for shift in dp_shifts:
            to = dp_at(shift)
            remote(in_send.at[l, to["dp"]], in_recv.at[l, me_dp], in_at(l), to)
        in_recv[l, me_dp] = in_send[l, me_dp]

    def earlier(l):
        lens = jnp.zeros((rows, LANES), jnp.int32)
        for b in range(rows):
            lens = jnp.where(sub == b, counts[b], lens)
        for b in range(rows):
            for r in range(roles):
                hist_f[pl.ds((b * roles + r) * width_back, width_back), :] = hist_v[
                    l, b, r
                ].astype(F32)
        for r in range(roles):
            total = jnp.zeros((rows, LANES), F32)
            for j in range(width_back):
                past = hist_f[pl.ds(r * width_back + j, rows, stride=roles * width_back), :]
                live = jnp.where(lens >= width_back - j, past, 0.0)
                total = total + live * taps[j, r, l : l + 1].astype(F32)
                if j:
                    win_f[
                        l, pl.ds(r * width_back + j - 1, rows, stride=roles * width_back), :
                    ] = past
            early_v[l, r] = total
        diagonal = lax.broadcasted_iota(jnp.int32, (rows, rows), 0) == lax.broadcasted_iota(
            jnp.int32, (rows, rows), 1
        )
        extra = [
            jnp.sum(jnp.where(diagonal, extra_log[l, k : k + 1, :], 0.0), axis=1, keepdims=True)
            for k in range(heads)
        ]
        fixed_v[l, 0] = jnp.where(first_head, extra[0], extra[1])
        fixed_v[l, 1] = jnp.exp(spread(decay_log, l))
        fixed_v[l, 2] = spread(step_bias, l)
        fixed_v[l, 3] = spread(direct_gain, l)

    def window(l):
        for b in range(rows):
            for r in range(roles):
                window_out[l, b, r] = win_f[
                    l, pl.ds((b * roles + r) * width_back, width_back), :
                ].astype(BF16)

    def mixer(l):
        with jax.named_scope(f"mixer{l}"):
            arrived = jnp.sum(in_recv[l].astype(F32), axis=0)
            stats = arrived[4]

            def stat(k):
                both = jnp.where((lane == k) | (lane == k + STAT), stats, 0.0)
                return jnp.sum(both, axis=1, keepdims=True)

            inverse = lax.rsqrt(stat(heads) / D + EPSILON)
            current = [(inverse * arrived[k]).astype(BF16).astype(F32) for k in range(roles)]
            gate = (inverse * arrived[3]).astype(BF16).astype(F32)
            step = jnp.where(first_head, stat(0), stat(1)) * inverse
            step = step.astype(BF16).astype(F32)
            value, inkey, readkey = [
                jax.nn.silu(
                    early_v[l, r] + current[r] * taps[width_back, r, l : l + 1].astype(F32)
                )
                for r in range(roles)
            ]
            rate = jax.nn.softplus(step + fixed_v[l, 2])
            decay = jnp.exp(-rate * fixed_v[l, 1] + fixed_v[l, 0])
            gain = rate * value
            gain_t = jnp.transpose(jnp.concatenate([gain] * (LANES // rows), axis=0))
            lane_sq = lax.broadcasted_iota(jnp.int32, (head_dim, LANES), 1)
            reads = [jnp.zeros((head_dim, LANES), F32) for _ in range(heads)]
            for b in range(rows):
                key_b = jnp.broadcast_to(inkey[b : b + 1], (head_dim, LANES))
                read_b = jnp.broadcast_to(readkey[b : b + 1], (head_dim, LANES))
                for k in range(heads):
                    decay_b = decay[b : b + 1, k * head_dim : k * head_dim + 1]
                    column = gain_t[k * head_dim : (k + 1) * head_dim, b : b + 1]
                    new = decay_b * state_v[l, b, k] + column * key_b
                    state_out[l, b, k] = new
                    read = jnp.sum(new * read_b, axis=1, keepdims=True)
                    reads[k] = jnp.where(lane_sq == b, read, reads[k])
            readout = jnp.transpose(jnp.concatenate(reads, axis=0))[0:rows]
            readout = readout + fixed_v[l, 3] * value
            gated = readout * jax.nn.silu(gate)
            scale = lax.rsqrt(jnp.mean(gated * gated, axis=1, keepdims=True) + EPSILON)
            normed = (gated * scale * out_gain[l : l + 1, :]).astype(BF16)
            if l + 1 < layers:
                wide_recv[me_quarter * n_dp + me_dp] = normed
            else:
                mix_recv[me_dp] = normed
            for r in range(roles):
                win_f[
                    l, pl.ds((r + 1) * width_back - 1, rows, stride=roles * width_back), :
                ] = current[r]

    def send_mix(l):
        if l + 1 < layers:
            here = wide_recv.at[me_quarter * n_dp + me_dp]
            for shift in dp_shifts:
                for near in range(1, blocks):
                    remote(here, here, mix_at(l), near_at(near) | dp_at(shift))
            for near in range(1, blocks):
                remote(here, here, mix_at(l), near_at(near))
        else:
            here = mix_recv.at[me_dp]
        for shift in dp_shifts:
            remote(here, here, mix_at(l), dp_at(shift))

    def wait_mix(l, sem):
        if l + 1 < layers:
            total_wait(wide_recv, blocks * n_dp - 1, sem)
        else:
            total_wait(mix_recv, n_dp - 1, sem)

    def send_weights():
        for near in range(1, blocks):
            quarter = lax.rem(me_quarter + near, blocks)
            columns = pl.ds(pl.multiple_of(quarter * LANES, LANES), LANES)
            remote(wo_v.at[0, :, columns], wo_near.at[me_quarter], weights_near, near_at(near))
        columns = pl.ds(pl.multiple_of(me_quarter * LANES, LANES), LANES)
        wo_near[me_quarter] = wo_v[0, :, columns]

    def reduce_all():
        with jax.named_scope("far_send"):
            mix = jnp.concatenate(
                [
                    jnp.concatenate(
                        [wide_recv[q * n_dp + i].astype(F32) for i in range(n_dp)], axis=0
                    ).astype(BF16)
                    for q in range(blocks)
                ],
                axis=1,
            )
            part = jnp.dot(
                mix, wo_near[...].reshape(-1, LANES), preferred_element_type=F32
            )
            far_recv[me_block] = part.astype(BF16)
            pl.semaphore_wait(know_sem.at[1], 2)
            for step in range(far // 2, 0, -1):
                for shift in sorted({step, far - step}):
                    to = tp_at(shift * blocks)
                    remote(far_recv.at[me_block], far_recv.at[me_block], far_sum, to)
            h = h_v[:, pl.ds(pl.multiple_of(me_quarter * LANES, LANES), LANES)].astype(F32)
        with jax.named_scope("far_wait"):
            total_wait(far_recv, far - 1, recv_sem.at[far_sum])
        with jax.named_scope("near_all"):
            mine = (h + jnp.sum(far_recv[...].astype(F32), axis=0)).astype(BF16)
            own_recv[me_quarter] = mine
            for shift in range(1, blocks):
                remote(own_recv.at[me_quarter], own_recv.at[me_quarter], near_all, near_at(shift))
        with jax.named_scope("near_all_wait"):
            total_wait(own_recv, blocks - 1, recv_sem.at[near_all])
        return jnp.concatenate([own_recv[j].astype(F32) for j in range(blocks)], axis=1)

    def reduce_rows(l):
        with jax.named_scope("ring_send"):
            kept_rows = batch // n_tp
            mix = jnp.concatenate(
                [mix_recv[i].astype(F32) for i in range(n_dp)], axis=0
            ).astype(BF16)
            part = jnp.dot(mix, wo_v[l], preferred_element_type=F32)
            for j in range(blocks):
                tile_f[pl.ds(j, batch, stride=blocks), :] = part[:, j * LANES : (j + 1) * LANES]
            for i in range(n_tp):
                part_send[i] = tile_f[i * 8 : (i + 1) * 8, :].astype(BF16)

            def to(shift):
                at = lax.rem(me_tp + shift, n_tp)
                remote(part_send.at[at], part_recv.at[me_tp], ring_sum, {"tp": at})

            def pair(step, _):
                to(n_tp // 2 - step)
                to(n_tp // 2 + step)
                return 0

            to(n_tp // 2)
            lax.fori_loop(1, n_tp // 2, pair, 0)
            part_recv[me_tp] = part_send[me_tp]
        with jax.named_scope("ring_wait"):
            at_row = lax.broadcasted_iota(jnp.int32, (8, batch), 0)
            at_col = lax.broadcasted_iota(jnp.int32, (8, batch), 1)
            pick = ((at_col == kept_rows * me_tp + at_row) & (at_row < kept_rows)).astype(BF16)
            h = jnp.concatenate([own_recv[j] for j in range(blocks)], axis=1)
            kept = jnp.dot(pick, h, preferred_element_type=F32)[0:kept_rows]
            window(l)
            total_wait(part_recv, n_tp - 1, recv_sem.at[ring_sum])
        with jax.named_scope("ring_sum"):
            tile_f[0:8, :] = jnp.sum(part_recv[...].astype(F32), axis=0)
            update = jnp.concatenate(
                [tile_f[pl.ds(j, kept_rows, stride=blocks), :] for j in range(blocks)], axis=1
            )
            hidden_out[...] = (kept + update).astype(BF16)

    with jax.named_scope("load_wait"):
        for copy in h_load:
            copy.wait()
    project(0, h_v[...].astype(F32))
    with jax.named_scope("barrier"):
        pl.semaphore_wait(barrier, n_dp - 1 + 2 * blocks)
    with jax.named_scope("send_in0"):
        send_in(0)
        for to in (blocks, -blocks):
            signal(know_sem.at[0], tp_at(to))
        wo_loads[0].wait()
        send_weights()
        for copy in small_loads:
            copy.wait()
        for l in range(layers):
            earlier(l)
        state_loads[0].wait()

    for l in range(layers):
        with jax.named_scope(f"in_wait{l}"):
            total_wait(in_recv.at[l], n_dp - 1, recv_sem.at[in_at(l)])
        mixer(l)
        with jax.named_scope(f"send_mix{l}"):
            send_mix(l)
            if l == 0:
                pl.semaphore_wait(know_sem.at[0], 2)
                for to in (2 * blocks, -2 * blocks):
                    signal(know_sem.at[1], tp_at(to))
                window(l)
                total_wait(wo_near, blocks - 1, recv_sem.at[weights_near])
                for copy in w_loads[1]:
                    copy.wait()
        with jax.named_scope(f"mix_wait{l}"):
            wait_mix(l, recv_sem.at[mix_at(l)])
        if l + 1 < layers:
            project(l + 1, reduce_all())
            with jax.named_scope(f"send_in{l + 1}"):
                send_in(l + 1)
                state_loads[l + 1].wait()
                wo_loads[l + 1].wait()
        else:
            reduce_rows(l)

    with jax.named_scope("end"):
        for l in range(layers):
            total_wait(in_send.at[l], n_dp - 1, send_sem.at[in_at(l)])
            wait_mix(l, send_sem.at[mix_at(l)])
        total_wait(wo_near, blocks - 1, send_sem.at[weights_near])
        total_wait(far_recv, far - 1, send_sem.at[far_sum])
        total_wait(own_recv, blocks - 1, send_sem.at[near_all])
        total_wait(part_send, n_tp - 1, send_sem.at[ring_sum])


def write_out(pieces, hidden_v, states_v, windows_v, hidden, states, windows, sem):
    copies = [
        pltpu.make_async_copy(hidden_v, hidden, sem.at[0]),
        pltpu.make_async_copy(windows_v, windows, sem.at[1]),
    ]
    layers, batch = states.shape[:2]
    step = layers * batch // pieces
    for p in range(pieces):
        l, b = divmod(p * step, batch)
        part = pl.ds(b, step)
        copies.append(
            pltpu.make_async_copy(states_v.at[l, part], states.at[l, part], sem.at[2 + p])
        )
    for copy in copies:
        copy.start()
    for copy in copies:
        copy.wait()


def body(n_tp, n_dp, *args):
    args = list(args)
    args[7] = jnp.transpose(args[7], (0, 2, 1))
    args[8] = jnp.transpose(args[8], (1, 2, 0, 3))
    args[9] = jnp.transpose(args[9], (0, 1, 3, 2, 4))
    args[13] = jnp.transpose(args[13], (0, 2, 1))
    h, w_value, history, state, w_out = (args[k] for k in (0, 3, 9, 14, 16))
    layers, feats, chans = w_value.shape
    batch = h.shape[0]
    rows = batch // n_dp
    roles, width_back = history.shape[2:4]
    blocks = feats // LANES
    vmem = pl.BlockSpec(memory_space=pltpu.VMEM)
    hbm = pl.BlockSpec(memory_space=pl.ANY)
    kept = pltpu.VMEM((batch // n_tp, feats), BF16), pltpu.VMEM(state.shape, F32), pltpu.VMEM(
        history.shape, BF16
    )
    in_vmem = pl.pallas_call(
        functools.partial(kernel, n_tp, n_dp),
        out_shape=kept,
        in_specs=[hbm] * len(args),
        out_specs=(vmem, vmem, vmem),
        scratch_shapes=[
            pltpu.SMEM(args[1].shape, args[1].dtype),
            *(pltpu.VMEM(args[k].shape, args[k].dtype) for k in (2, 7, 8)),
            *(pltpu.SMEM(args[k].shape, args[k].dtype) for k in (10, 11, 12)),
            *(pltpu.VMEM(args[k].shape, args[k].dtype) for k in (13, 15)),
            pltpu.VMEM((batch, feats), BF16),
            pltpu.VMEM((layers, feats, 4 * chans), BF16),
            pltpu.VMEM(w_out.shape, BF16),
            pltpu.VMEM(history.shape, BF16),
            pltpu.VMEM(state.shape, F32),
            pltpu.VMEM((rows * roles * width_back, LANES), F32),
            pltpu.VMEM((layers, rows * roles * width_back, LANES), F32),
            pltpu.VMEM((layers, roles, rows, LANES), F32),
            pltpu.VMEM((layers, 4, rows, LANES), F32),
            pltpu.VMEM((n_tp * 8, LANES), F32),
            pltpu.VMEM((layers, n_dp, 5, rows, LANES), BF16),
            pltpu.VMEM((layers, n_dp, 5, rows, LANES), BF16),
            pltpu.VMEM((n_dp, rows, LANES), BF16),
            pltpu.VMEM((blocks * n_dp, rows, LANES), BF16),
            pltpu.VMEM((blocks, chans, LANES), BF16),
            pltpu.VMEM((n_tp // blocks, batch, LANES), BF16),
            pltpu.VMEM((blocks, batch, LANES), BF16),
            pltpu.VMEM((n_tp, 8, LANES), BF16),
            pltpu.VMEM((n_tp, 8, LANES), BF16),
            pltpu.SemaphoreType.DMA((3 + 3 * layers,)),
            pltpu.SemaphoreType.DMA((2 * layers + 4,)),
            pltpu.SemaphoreType.DMA((2 * layers + 4,)),
            pltpu.SemaphoreType.REGULAR((2,)),
        ],
        compiler_params=pltpu.CompilerParams(collective_id=0, has_side_effects=True),
    )(*args)
    pieces = 4
    hidden, states, windows = pl.pallas_call(
        functools.partial(write_out, pieces),
        out_shape=tuple(jax.ShapeDtypeStruct(k.shape, k.dtype) for k in in_vmem),
        in_specs=[vmem] * 3,
        out_specs=(hbm, hbm, hbm),
        scratch_shapes=[pltpu.SemaphoreType.DMA((2 + pieces,))],
    )(*(pltpu.with_memory_space_constraint(k, pltpu.VMEM) for k in in_vmem))
    return hidden, states, jnp.transpose(windows, (0, 1, 3, 2, 4))


def solution(mesh):
    placed = (
        P("grp", "dp"),
        P(("grp", "dp")),
        P(None, "dp"),
        P(None, "dp", "tp"),
        P(None, "dp", "tp"),
        P(None, "dp", "tp"),
        P(None, "dp", "tp"),
        P(None, "dp", None),
        P(None, None, None, "tp"),
        P(None, ("grp", "dp"), None, None, "tp"),
        P(None, "tp"),
        P(None, "tp"),
        P(None, "tp"),
        P(None, ("grp", "dp"), "tp"),
        P(None, ("grp", "dp"), "tp", None, None),
        P(None, "tp"),
        P(None, "tp", "dp"),
    )
    return jax.shard_map(
        functools.partial(body, mesh.shape["tp"], mesh.shape["dp"]),
        mesh=mesh,
        in_specs=placed,
        out_specs=(
            P(("grp", "tp"), "dp"),
            P(None, ("grp", "dp"), "tp", None, None),
            P(None, ("grp", "dp"), None, None, "tp"),
        ),
        check_vma=False,
    )
```

```python
import functools

import jax
import jax.numpy as jnp
from jax import lax
from jax.experimental import pallas as pl
from jax.experimental.pallas import tpu as pltpu
from jax.sharding import PartitionSpec as P

D = 4096
EPSILON = 1e-06
MESH = pl.DeviceIdType.MESH
F32 = jnp.float32
BF16 = jnp.bfloat16
LANES = 128
STAT = 3


def total_wait(buffer, count, sem):
    part = buffer.at[pl.ds(0, count)]
    pltpu.make_async_copy(part, part, sem).wait()


def kernel(
    n_tp,
    n_dp,
    h_in,
    counts_in,
    in_gain_in,
    w_value,
    w_inkey,
    w_readkey,
    w_gate,
    w_step_in,
    taps_in,
    history,
    step_bias_in,
    decay_log_in,
    direct_gain_in,
    extra_log_in,
    state_in,
    out_gain_in,
    w_out,
    hidden_out,
    state_out,
    window_out,
    counts,
    in_gain,
    w_step,
    taps,
    step_bias,
    decay_log,
    direct_gain,
    extra_log,
    out_gain,
    h_v,
    wp_v,
    wo_v,
    hist_v,
    state_v,
    hist_f,
    win_f,
    early_v,
    fixed_v,
    tile_f,
    in_send,
    in_recv,
    mix_recv,
    wide_recv,
    wo_near,
    far_recv,
    own_recv,
    part_send,
    part_recv,
    load_sem,
    send_sem,
    recv_sem,
    know_sem,
):
    layers = w_out.shape[0]
    batch, feats = h_in.shape
    rows = batch // n_dp
    blocks = feats // LANES
    head_dim = state_in.shape[3]
    heads = state_in.shape[2]
    roles, width_back = history.shape[2:4]
    far = n_tp // blocks
    me_tp = lax.axis_index("tp")
    me_dp = lax.axis_index("dp")
    me_block = me_tp // blocks
    me_quarter = lax.rem(me_tp, blocks)

    def tp_at(shift):
        return {"tp": lax.rem(me_tp + (n_tp + shift), n_tp)}

    def dp_at(shift):
        return {"dp": lax.rem(me_dp + shift, n_dp)}

    def near_at(shift):
        return {"tp": me_block * blocks + lax.rem(me_quarter + shift, blocks)}

    def remote(source, target, sem, to):
        pltpu.make_async_remote_copy(
            src_ref=source,
            dst_ref=target,
            send_sem=send_sem.at[sem],
            recv_sem=recv_sem.at[sem],
            device_id=to,
            device_id_type=MESH,
        ).start()

    def signal(sem, to):
        pl.semaphore_signal(sem, inc=1, device_id=to, device_id_type=MESH)

    in_at = lambda l: l
    mix_at = lambda l: layers + l
    weights_near, far_sum, near_all, ring_sum = (2 * layers + k for k in range(4))
    dp_shifts = sorted(range(1, n_dp), key=lambda s: abs(s - n_dp // 2))

    def load(source, target, sem):
        copy = pltpu.make_async_copy(source, target, load_sem.at[sem])
        copy.start()
        return copy

    def load_products(l):
        return [
            load(w.at[l], wp_v.at[l, :, pl.ds(k * LANES, LANES)], 1 + l)
            for k, w in enumerate((w_value, w_inkey, w_readkey, w_gate))
        ]

    h_load = [load(h_in, h_v, 0), load(in_gain_in, in_gain, 0)]
    w_loads = [load_products(0)]
    step_load = load(w_step_in, w_step, 1 + layers)

    barrier = pltpu.get_barrier_semaphore()
    for shift in range(1, n_dp):
        signal(barrier, dp_at(shift))
    for shift in range(1, blocks + 1):
        for to in (shift, -shift):
            signal(barrier, tp_at(to))

    lane = lax.broadcasted_iota(jnp.int32, (rows, LANES), 1)
    lane_all = lax.broadcasted_iota(jnp.int32, (batch, LANES), 1)
    sub = lax.broadcasted_iota(jnp.int32, (rows, LANES), 0)
    first_head = lane < head_dim
    unit = (
        lax.broadcasted_iota(jnp.int32, (LANES, LANES), 0)
        == lax.broadcasted_iota(jnp.int32, (LANES, LANES), 1)
    ).astype(BF16)

    def halves(x):
        high = x.astype(BF16)
        return high, (x - high.astype(F32)).astype(BF16)

    def spread(values, in_layer):
        return jnp.where(first_head, values[in_layer, 0], values[in_layer, 1])

    def project(l, h):
        with jax.named_scope(f"proj{l}"):
            squares = jnp.sum(h * h, axis=1, keepdims=True)
            scaled = (h * in_gain[l : l + 1, :]).astype(BF16)
            if l == 0:
                step_load.wait()
            steps = lax.dot_general(
                scaled, w_step[l], (((1,), (1,)), ((), ())), preferred_element_type=F32
            )
            lane_step = lax.broadcasted_iota(jnp.int32, steps.shape, 1)
            wanted = [
                jnp.sum(
                    jnp.where(lane_step == me_tp * heads + k, steps, 0.0), axis=1, keepdims=True
                )
                for k in range(heads)
            ] + [squares]
            if l == 0:
                for copy in w_loads[l]:
                    copy.wait()
            part = jnp.dot(scaled, wp_v[l], preferred_element_type=F32)
            stats = jnp.zeros((batch, LANES), F32)
            for k, v in enumerate(wanted):
                high = v.astype(BF16).astype(F32)
                stats = jnp.where(lane_all == k, high, stats)
                stats = jnp.where(lane_all == k + STAT, v - high, stats)
            for i in range(n_dp):
                at = slice(i * rows, (i + 1) * rows)
                for k in range(4):
                    in_send[l, i, k] = part[at, k * LANES : (k + 1) * LANES].astype(BF16)
                in_send[l, i, 4] = stats[at].astype(BF16)

    def send_in(l):
        for shift in dp_shifts:
            to = dp_at(shift)
            remote(in_send.at[l, to["dp"]], in_recv.at[l, me_dp], in_at(l), to)
        in_recv[l, me_dp] = in_send[l, me_dp]

    def earlier(l):
        lens = jnp.zeros((rows, LANES), jnp.int32)
        for b in range(rows):
            lens = jnp.where(sub == b, counts[b], lens)
        for b in range(rows):
            for r in range(roles):
                hist_f[pl.ds((b * roles + r) * width_back, width_back), :] = hist_v[
                    l, b, r
                ].astype(F32)
        for r in range(roles):
            total = jnp.zeros((rows, LANES), F32)
            for j in range(width_back):
                past = hist_f[pl.ds(r * width_back + j, rows, stride=roles * width_back), :]
                live = jnp.where(lens >= width_back - j, past, 0.0)
                total = total + live * taps[j, r, l : l + 1].astype(F32)
                if j:
                    win_f[
                        l, pl.ds(r * width_back + j - 1, rows, stride=roles * width_back), :
                    ] = past
            early_v[l, r] = total
        diagonal = lax.broadcasted_iota(jnp.int32, (rows, rows), 0) == lax.broadcasted_iota(
            jnp.int32, (rows, rows), 1
        )
        extra = [
            jnp.sum(jnp.where(diagonal, extra_log[l, k : k + 1, :], 0.0), axis=1, keepdims=True)
            for k in range(heads)
        ]
        fixed_v[l, 0] = jnp.where(first_head, extra[0], extra[1])
        fixed_v[l, 1] = jnp.exp(spread(decay_log, l))
        fixed_v[l, 2] = spread(step_bias, l)
        fixed_v[l, 3] = spread(direct_gain, l)

    def window(l):
        for b in range(rows):
            for r in range(roles):
                window_out[l, b, r] = win_f[
                    l, pl.ds((b * roles + r) * width_back, width_back), :
                ].astype(BF16)

    def mixer(l):
        with jax.named_scope(f"mixer{l}"):
            arrived = jnp.sum(in_recv[l].astype(F32), axis=0)
            stats = arrived[4]

            def stat(k):
                both = jnp.where((lane == k) | (lane == k + STAT), stats, 0.0)
                return jnp.sum(both, axis=1, keepdims=True)

            inverse = lax.rsqrt(stat(heads) / D + EPSILON)
            current = [(inverse * arrived[k]).astype(BF16).astype(F32) for k in range(roles)]
            gate = (inverse * arrived[3]).astype(BF16).astype(F32)
            step = jnp.where(first_head, stat(0), stat(1)) * inverse
            step = step.astype(BF16).astype(F32)
            value, inkey, readkey = [
                jax.nn.silu(
                    early_v[l, r] + current[r] * taps[width_back, r, l : l + 1].astype(F32)
                )
                for r in range(roles)
            ]
            rate = jax.nn.softplus(step + fixed_v[l, 2])
            decay = jnp.exp(-rate * fixed_v[l, 1] + fixed_v[l, 0])
            gain = rate * value
            high, low = halves(gain)
            none = jnp.zeros((LANES - 3 * rows, LANES), BF16)
            parts = jnp.concatenate([high, high, low, none], axis=0)
            columns = lax.dot_general(
                unit, parts, (((1,), (1,)), ((), ())), preferred_element_type=F32
            )
            lane_sq = lax.broadcasted_iota(jnp.int32, (LANES, LANES), 1)
            left = jnp.concatenate(
                [jnp.where(lane_sq % rows == b, columns, 0.0).astype(BF16) for b in range(rows)],
                axis=0,
            )
            high, low = halves(inkey)
            right = jnp.concatenate([high, low, high, none], axis=0)
            outer = jnp.dot(left, right, preferred_element_type=F32)
            reader = readkey.astype(BF16)
            fades = [
                jnp.broadcast_to(decay[:, k * head_dim : k * head_dim + 1], (rows, LANES))
                for k in range(heads)
            ]
            readout = jnp.zeros((rows, LANES), F32)
            for b in range(rows):
                news = []
                for k in range(heads):
                    at = (b * heads + k) * head_dim
                    new = fades[k][b : b + 1] * state_v[l, b, k] + outer[at : at + head_dim]
                    state_out[l, b, k] = new
                    news.append(new.astype(BF16))
                read = lax.dot_general(
                    reader,
                    jnp.concatenate(news, axis=0),
                    (((1,), (1,)), ((), ())),
                    preferred_element_type=F32,
                )
                readout = jnp.where(sub == b, read, readout)
            readout = readout + fixed_v[l, 3] * value
            gated = readout * jax.nn.silu(gate)
            scale = lax.rsqrt(jnp.mean(gated * gated, axis=1, keepdims=True) + EPSILON)
            normed = (gated * scale * out_gain[l : l + 1, :]).astype(BF16)
            if l + 1 < layers:
                wide_recv[me_quarter * n_dp + me_dp] = normed
            else:
                mix_recv[me_dp] = normed
            for r in range(roles):
                win_f[
                    l, pl.ds((r + 1) * width_back - 1, rows, stride=roles * width_back), :
                ] = current[r]

    def send_mix(l):
        if l + 1 < layers:
            here = wide_recv.at[me_quarter * n_dp + me_dp]
            for shift in dp_shifts:
                for near in range(1, blocks):
                    remote(here, here, mix_at(l), near_at(near) | dp_at(shift))
            for near in range(1, blocks):
                remote(here, here, mix_at(l), near_at(near))
        else:
            here = mix_recv.at[me_dp]
        for shift in dp_shifts:
            remote(here, here, mix_at(l), dp_at(shift))

    def wait_mix(l, sem):
        if l + 1 < layers:
            total_wait(wide_recv, blocks * n_dp - 1, sem)
        else:
            total_wait(mix_recv, n_dp - 1, sem)

    def send_weights():
        for near in range(1, blocks):
            quarter = lax.rem(me_quarter + near, blocks)
            columns = pl.ds(pl.multiple_of(quarter * LANES, LANES), LANES)
            remote(wo_v.at[0, :, columns], wo_near.at[me_quarter], weights_near, near_at(near))
        columns = pl.ds(pl.multiple_of(me_quarter * LANES, LANES), LANES)
        wo_near[me_quarter] = wo_v[0, :, columns]

    def reduce_all():
        with jax.named_scope("far_send"):
            mix = jnp.concatenate(
                [
                    jnp.concatenate(
                        [wide_recv[q * n_dp + i].astype(F32) for i in range(n_dp)], axis=0
                    ).astype(BF16)
                    for q in range(blocks)
                ],
                axis=1,
            )
            part = jnp.dot(
                mix, wo_near[...].reshape(-1, LANES), preferred_element_type=F32
            )
            far_recv[me_block] = part.astype(BF16)
            pl.semaphore_wait(know_sem.at[1], 2)
            for step in range(far // 2, 0, -1):
                for shift in sorted({step, far - step}):
                    to = tp_at(shift * blocks)
                    remote(far_recv.at[me_block], far_recv.at[me_block], far_sum, to)
            h = h_v[:, pl.ds(pl.multiple_of(me_quarter * LANES, LANES), LANES)].astype(F32)
        with jax.named_scope("far_wait"):
            total_wait(far_recv, far - 1, recv_sem.at[far_sum])
        with jax.named_scope("near_all"):
            mine = (h + jnp.sum(far_recv[...].astype(F32), axis=0)).astype(BF16)
            own_recv[me_quarter] = mine
            for shift in range(1, blocks):
                remote(own_recv.at[me_quarter], own_recv.at[me_quarter], near_all, near_at(shift))
        with jax.named_scope("near_all_wait"):
            total_wait(own_recv, blocks - 1, recv_sem.at[near_all])
        return jnp.concatenate([own_recv[j].astype(F32) for j in range(blocks)], axis=1)

    def reduce_rows(l):
        with jax.named_scope("ring_send"):
            kept_rows = batch // n_tp
            mix = jnp.concatenate(
                [mix_recv[i].astype(F32) for i in range(n_dp)], axis=0
            ).astype(BF16)
            part = jnp.dot(mix, wo_v[l], preferred_element_type=F32)
            for j in range(blocks):
                tile_f[pl.ds(j, batch, stride=blocks), :] = part[:, j * LANES : (j + 1) * LANES]
            for i in range(n_tp):
                part_send[i] = tile_f[i * 8 : (i + 1) * 8, :].astype(BF16)

            def to(shift):
                at = lax.rem(me_tp + shift, n_tp)
                remote(part_send.at[at], part_recv.at[me_tp], ring_sum, {"tp": at})

            def pair(step, _):
                to(n_tp // 2 - step)
                to(n_tp // 2 + step)
                return 0

            to(n_tp // 2)
            lax.fori_loop(1, n_tp // 2, pair, 0)
            part_recv[me_tp] = part_send[me_tp]
        with jax.named_scope("ring_wait"):
            at_row = lax.broadcasted_iota(jnp.int32, (8, batch), 0)
            at_col = lax.broadcasted_iota(jnp.int32, (8, batch), 1)
            pick = ((at_col == kept_rows * me_tp + at_row) & (at_row < kept_rows)).astype(BF16)
            h = jnp.concatenate([own_recv[j] for j in range(blocks)], axis=1)
            kept = jnp.dot(pick, h, preferred_element_type=F32)[0:kept_rows]
            window(l)
            total_wait(part_recv, n_tp - 1, recv_sem.at[ring_sum])
        with jax.named_scope("ring_sum"):
            tile_f[0:8, :] = jnp.sum(part_recv[...].astype(F32), axis=0)
            update = jnp.concatenate(
                [tile_f[pl.ds(j, kept_rows, stride=blocks), :] for j in range(blocks)], axis=1
            )
            hidden_out[...] = (kept + update).astype(BF16)

    with jax.named_scope("load_wait"):
        for copy in h_load:
            copy.wait()
    project(0, h_v[...].astype(F32))
    with jax.named_scope("barrier"):
        pl.semaphore_wait(barrier, n_dp - 1 + 2 * blocks)
    with jax.named_scope("send_in0"):
        send_in(0)
        for to in (blocks, -blocks):
            signal(know_sem.at[0], tp_at(to))
        small_loads = [
            load(source, target, 2 + layers)
            for source, target in (
                (history, hist_v),
                (counts_in, counts),
                (taps_in, taps),
                (step_bias_in, step_bias),
                (decay_log_in, decay_log),
                (direct_gain_in, direct_gain),
                (extra_log_in, extra_log),
                (out_gain_in, out_gain),
            )
        ]
        state_loads = [load(state_in.at[0], state_v.at[0], 3 + layers)]
        wo_loads = [load(w_out.at[0], wo_v.at[0], 3 + 2 * layers)]
        for l in range(1, layers):
            w_loads.append(load_products(l))
            state_loads.append(load(state_in.at[l], state_v.at[l], 3 + layers + l))
            wo_loads.append(load(w_out.at[l], wo_v.at[l], 3 + 2 * layers + l))
        for copy in small_loads:
            copy.wait()
        for l in range(layers):
            earlier(l)
        wo_loads[0].wait()
        send_weights()
        state_loads[0].wait()

    for l in range(layers):
        with jax.named_scope(f"in_wait{l}"):
            total_wait(in_recv.at[l], n_dp - 1, recv_sem.at[in_at(l)])
        if l == 0:
            with jax.named_scope("know"):
                pl.semaphore_wait(know_sem.at[0], 2)
                for to in (2 * blocks, -2 * blocks):
                    signal(know_sem.at[1], tp_at(to))
        mixer(l)
        with jax.named_scope(f"send_mix{l}"):
            send_mix(l)
            if l == 0:
                window(l)
                total_wait(wo_near, blocks - 1, recv_sem.at[weights_near])
                for copy in w_loads[1]:
                    copy.wait()
        with jax.named_scope(f"mix_wait{l}"):
            wait_mix(l, recv_sem.at[mix_at(l)])
        if l + 1 < layers:
            project(l + 1, reduce_all())
            with jax.named_scope(f"send_in{l + 1}"):
                send_in(l + 1)
                state_loads[l + 1].wait()
                wo_loads[l + 1].wait()
        else:
            reduce_rows(l)

    with jax.named_scope("end"):
        for l in range(layers):
            total_wait(in_send.at[l], n_dp - 1, send_sem.at[in_at(l)])
            wait_mix(l, send_sem.at[mix_at(l)])
        total_wait(wo_near, blocks - 1, send_sem.at[weights_near])
        total_wait(far_recv, far - 1, send_sem.at[far_sum])
        total_wait(own_recv, blocks - 1, send_sem.at[near_all])
        total_wait(part_send, n_tp - 1, send_sem.at[ring_sum])


def write_out(pieces, hidden_v, states_v, windows_v, hidden, states, windows, sem):
    copies = [
        pltpu.make_async_copy(hidden_v, hidden, sem.at[0]),
        pltpu.make_async_copy(windows_v, windows, sem.at[1]),
    ]
    layers, batch = states.shape[:2]
    step = layers * batch // pieces
    for p in range(pieces):
        l, b = divmod(p * step, batch)
        part = pl.ds(b, step)
        copies.append(
            pltpu.make_async_copy(states_v.at[l, part], states.at[l, part], sem.at[2 + p])
        )
    for copy in copies:
        copy.start()
    for copy in copies:
        copy.wait()


def body(n_tp, n_dp, *args):
    args = list(args)
    args[7] = jnp.transpose(args[7], (0, 2, 1))
    args[8] = jnp.transpose(args[8], (1, 2, 0, 3))
    args[9] = jnp.transpose(args[9], (0, 1, 3, 2, 4))
    args[13] = jnp.transpose(args[13], (0, 2, 1))
    h, w_value, history, state, w_out = (args[k] for k in (0, 3, 9, 14, 16))
    layers, feats, chans = w_value.shape
    batch = h.shape[0]
    rows = batch // n_dp
    roles, width_back = history.shape[2:4]
    blocks = feats // LANES
    vmem = pl.BlockSpec(memory_space=pltpu.VMEM)
    hbm = pl.BlockSpec(memory_space=pl.ANY)
    kept = pltpu.VMEM((batch // n_tp, feats), BF16), pltpu.VMEM(state.shape, F32), pltpu.VMEM(
        history.shape, BF16
    )
    in_vmem = pl.pallas_call(
        functools.partial(kernel, n_tp, n_dp),
        out_shape=kept,
        in_specs=[hbm] * len(args),
        out_specs=(vmem, vmem, vmem),
        scratch_shapes=[
            pltpu.SMEM(args[1].shape, args[1].dtype),
            *(pltpu.VMEM(args[k].shape, args[k].dtype) for k in (2, 7, 8)),
            *(pltpu.SMEM(args[k].shape, args[k].dtype) for k in (10, 11, 12)),
            *(pltpu.VMEM(args[k].shape, args[k].dtype) for k in (13, 15)),
            pltpu.VMEM((batch, feats), BF16),
            pltpu.VMEM((layers, feats, 4 * chans), BF16),
            pltpu.VMEM(w_out.shape, BF16),
            pltpu.VMEM(history.shape, BF16),
            pltpu.VMEM(state.shape, F32),
            pltpu.VMEM((rows * roles * width_back, LANES), F32),
            pltpu.VMEM((layers, rows * roles * width_back, LANES), F32),
            pltpu.VMEM((layers, roles, rows, LANES), F32),
            pltpu.VMEM((layers, 4, rows, LANES), F32),
            pltpu.VMEM((n_tp * 8, LANES), F32),
            pltpu.VMEM((layers, n_dp, 5, rows, LANES), BF16),
            pltpu.VMEM((layers, n_dp, 5, rows, LANES), BF16),
            pltpu.VMEM((n_dp, rows, LANES), BF16),
            pltpu.VMEM((blocks * n_dp, rows, LANES), BF16),
            pltpu.VMEM((blocks, chans, LANES), BF16),
            pltpu.VMEM((n_tp // blocks, batch, LANES), BF16),
            pltpu.VMEM((blocks, batch, LANES), BF16),
            pltpu.VMEM((n_tp, 8, LANES), BF16),
            pltpu.VMEM((n_tp, 8, LANES), BF16),
            pltpu.SemaphoreType.DMA((3 + 3 * layers,)),
            pltpu.SemaphoreType.DMA((2 * layers + 4,)),
            pltpu.SemaphoreType.DMA((2 * layers + 4,)),
            pltpu.SemaphoreType.REGULAR((2,)),
        ],
        compiler_params=pltpu.CompilerParams(collective_id=0, has_side_effects=True),
    )(*args)
    pieces = 4
    hidden, states, windows = pl.pallas_call(
        functools.partial(write_out, pieces),
        out_shape=tuple(jax.ShapeDtypeStruct(k.shape, k.dtype) for k in in_vmem),
        in_specs=[vmem] * 3,
        out_specs=(hbm, hbm, hbm),
        scratch_shapes=[pltpu.SemaphoreType.DMA((2 + pieces,))],
    )(*(pltpu.with_memory_space_constraint(k, pltpu.VMEM) for k in in_vmem))
    return hidden, states, jnp.transpose(windows, (0, 1, 3, 2, 4))


def solution(mesh):
    placed = (
        P("grp", "dp"),
        P(("grp", "dp")),
        P(None, "dp"),
        P(None, "dp", "tp"),
        P(None, "dp", "tp"),
        P(None, "dp", "tp"),
        P(None, "dp", "tp"),
        P(None, "dp", None),
        P(None, None, None, "tp"),
        P(None, ("grp", "dp"), None, None, "tp"),
        P(None, "tp"),
        P(None, "tp"),
        P(None, "tp"),
        P(None, ("grp", "dp"), "tp"),
        P(None, ("grp", "dp"), "tp", None, None),
        P(None, "tp"),
        P(None, "tp", "dp"),
    )
    return jax.shard_map(
        functools.partial(body, mesh.shape["tp"], mesh.shape["dp"]),
        mesh=mesh,
        in_specs=placed,
        out_specs=(
            P(("grp", "tp"), "dp"),
            P(None, ("grp", "dp"), "tp", None, None),
            P(None, ("grp", "dp"), None, None, "tp"),
        ),
        check_vma=False,
    )
```

```python
import functools

import jax
import jax.numpy as jnp
from jax import lax
from jax.experimental import pallas as pl
from jax.experimental.pallas import tpu as pltpu
from jax.sharding import PartitionSpec as P

D = 4096
EPSILON = 1e-06
MESH = pl.DeviceIdType.MESH
F32 = jnp.float32
BF16 = jnp.bfloat16
LANES = 128
STAT = 3


def total_wait(buffer, count, sem):
    part = buffer.at[pl.ds(0, count)]
    pltpu.make_async_copy(part, part, sem).wait()


def kernel(
    n_tp,
    n_dp,
    h_in,
    counts_in,
    in_gain_in,
    w_value,
    w_inkey,
    w_readkey,
    w_gate,
    w_step_in,
    taps_in,
    history,
    step_bias_in,
    decay_log_in,
    direct_gain_in,
    extra_log_in,
    state_in,
    out_gain_in,
    w_out,
    hidden_out,
    state_out,
    window_out,
    counts,
    in_gain,
    w_step,
    taps,
    step_bias,
    decay_log,
    direct_gain,
    extra_log,
    out_gain,
    h_v,
    wp_v,
    wo_v,
    hist_v,
    state_v,
    hist_f,
    win_f,
    early_v,
    fixed_v,
    tile_f,
    in_send,
    in_recv,
    mix_recv,
    wide_recv,
    wo_near,
    pair_v,
    far_recv,
    own_recv,
    part_send,
    part_recv,
    load_sem,
    send_sem,
    recv_sem,
    know_sem,
):
    layers = w_out.shape[0]
    batch, feats = h_in.shape
    rows = batch // n_dp
    blocks = feats // LANES
    head_dim = state_in.shape[3]
    heads = state_in.shape[2]
    roles, width_back = history.shape[2:4]
    far = n_tp // (2 * blocks)
    me_tp = lax.axis_index("tp")
    me_dp = lax.axis_index("dp")
    me_block = me_tp // blocks
    me_quarter = lax.rem(me_tp, blocks)
    me_pair = me_block // 2
    odd = lax.rem(me_block, 2)

    def tp_at(shift):
        return {"tp": lax.rem(me_tp + (n_tp + shift), n_tp)}

    def dp_at(shift):
        return {"dp": lax.rem(me_dp + shift, n_dp)}

    def near_at(shift):
        return {"tp": me_block * blocks + lax.rem(me_quarter + shift, blocks)}

    def remote(source, target, sem, to):
        pltpu.make_async_remote_copy(
            src_ref=source,
            dst_ref=target,
            send_sem=send_sem.at[sem],
            recv_sem=recv_sem.at[sem],
            device_id=to,
            device_id_type=MESH,
        ).start()

    def signal(sem, to):
        pl.semaphore_signal(sem, inc=1, device_id=to, device_id_type=MESH)

    in_at = lambda l: l
    mix_at = lambda l: layers + l
    weights_near, far_sum, near_all, ring_sum, pair_sum = (2 * layers + k for k in range(5))
    dp_shifts = sorted(range(1, n_dp), key=lambda s: abs(s - n_dp // 2))

    def load(source, target, sem):
        copy = pltpu.make_async_copy(source, target, load_sem.at[sem])
        copy.start()
        return copy

    def load_products(l):
        return [
            load(w.at[l], wp_v.at[l, :, pl.ds(k * LANES, LANES)], 1 + l)
            for k, w in enumerate((w_value, w_inkey, w_readkey, w_gate))
        ]

    h_load = [load(h_in, h_v, 0), load(in_gain_in, in_gain, 0)]
    w_loads = [load_products(0)]
    step_load = load(w_step_in, w_step, 1 + layers)

    barrier = pltpu.get_barrier_semaphore()
    for shift in range(1, n_dp):
        signal(barrier, dp_at(shift))
    for shift in range(1, blocks + 1):
        for to in (shift, -shift):
            signal(barrier, tp_at(to))

    lane = lax.broadcasted_iota(jnp.int32, (rows, LANES), 1)
    lane_all = lax.broadcasted_iota(jnp.int32, (batch, LANES), 1)
    sub = lax.broadcasted_iota(jnp.int32, (rows, LANES), 0)
    first_head = lane < head_dim
    unit = (
        lax.broadcasted_iota(jnp.int32, (LANES, LANES), 0)
        == lax.broadcasted_iota(jnp.int32, (LANES, LANES), 1)
    ).astype(BF16)

    def halves(x):
        high = x.astype(BF16)
        return high, (x - high.astype(F32)).astype(BF16)

    def spread(values, in_layer):
        return jnp.where(first_head, values[in_layer, 0], values[in_layer, 1])

    def project(l, h):
        with jax.named_scope(f"proj{l}"):
            squares = jnp.sum(h * h, axis=1, keepdims=True)
            scaled = (h * in_gain[l : l + 1, :]).astype(BF16)
            if l == 0:
                step_load.wait()
            steps = lax.dot_general(
                scaled, w_step[l], (((1,), (1,)), ((), ())), preferred_element_type=F32
            )
            lane_step = lax.broadcasted_iota(jnp.int32, steps.shape, 1)
            wanted = [
                jnp.sum(
                    jnp.where(lane_step == me_tp * heads + k, steps, 0.0), axis=1, keepdims=True
                )
                for k in range(heads)
            ] + [squares]
            if l == 0:
                for copy in w_loads[l]:
                    copy.wait()
            part = jnp.dot(scaled, wp_v[l], preferred_element_type=F32)
            stats = jnp.zeros((batch, LANES), F32)
            for k, v in enumerate(wanted):
                high = v.astype(BF16).astype(F32)
                stats = jnp.where(lane_all == k, high, stats)
                stats = jnp.where(lane_all == k + STAT, v - high, stats)
            for i in range(n_dp):
                at = slice(i * rows, (i + 1) * rows)
                for k in range(4):
                    in_send[l, i, k] = part[at, k * LANES : (k + 1) * LANES].astype(BF16)
                in_send[l, i, 4] = stats[at].astype(BF16)

    def send_in(l):
        for shift in dp_shifts:
            to = dp_at(shift)
            remote(in_send.at[l, to["dp"]], in_recv.at[l, me_dp], in_at(l), to)
        in_recv[l, me_dp] = in_send[l, me_dp]

    def earlier(l):
        lens = jnp.zeros((rows, LANES), jnp.int32)
        for b in range(rows):
            lens = jnp.where(sub == b, counts[b], lens)
        for b in range(rows):
            for r in range(roles):
                hist_f[pl.ds((b * roles + r) * width_back, width_back), :] = hist_v[
                    l, b, r
                ].astype(F32)
        for r in range(roles):
            total = jnp.zeros((rows, LANES), F32)
            for j in range(width_back):
                past = hist_f[pl.ds(r * width_back + j, rows, stride=roles * width_back), :]
                live = jnp.where(lens >= width_back - j, past, 0.0)
                total = total + live * taps[j, r, l : l + 1].astype(F32)
                if j:
                    win_f[
                        l, pl.ds(r * width_back + j - 1, rows, stride=roles * width_back), :
                    ] = past
            early_v[l, r] = total
        diagonal = lax.broadcasted_iota(jnp.int32, (rows, rows), 0) == lax.broadcasted_iota(
            jnp.int32, (rows, rows), 1
        )
        extra = [
            jnp.sum(jnp.where(diagonal, extra_log[l, k : k + 1, :], 0.0), axis=1, keepdims=True)
            for k in range(heads)
        ]
        fixed_v[l, 0] = jnp.where(first_head, extra[0], extra[1])
        fixed_v[l, 1] = jnp.exp(spread(decay_log, l))
        fixed_v[l, 2] = spread(step_bias, l)
        fixed_v[l, 3] = spread(direct_gain, l)

    def window(l):
        for b in range(rows):
            for r in range(roles):
                window_out[l, b, r] = win_f[
                    l, pl.ds((b * roles + r) * width_back, width_back), :
                ].astype(BF16)

    def mixer(l):
        with jax.named_scope(f"mixer{l}"):
            arrived = jnp.sum(in_recv[l].astype(F32), axis=0)
            stats = arrived[4]

            def stat(k):
                both = jnp.where((lane == k) | (lane == k + STAT), stats, 0.0)
                return jnp.sum(both, axis=1, keepdims=True)

            inverse = lax.rsqrt(stat(heads) / D + EPSILON)
            current = [(inverse * arrived[k]).astype(BF16).astype(F32) for k in range(roles)]
            gate = (inverse * arrived[3]).astype(BF16).astype(F32)
            step = jnp.where(first_head, stat(0), stat(1)) * inverse
            step = step.astype(BF16).astype(F32)
            value, inkey, readkey = [
                jax.nn.silu(
                    early_v[l, r] + current[r] * taps[width_back, r, l : l + 1].astype(F32)
                )
                for r in range(roles)
            ]
            rate = jax.nn.softplus(step + fixed_v[l, 2])
            decay = jnp.exp(-rate * fixed_v[l, 1] + fixed_v[l, 0])
            gain = rate * value
            high, low = halves(gain)
            none = jnp.zeros((LANES - 3 * rows, LANES), BF16)
            parts = jnp.concatenate([high, high, low, none], axis=0)
            columns = lax.dot_general(
                unit, parts, (((1,), (1,)), ((), ())), preferred_element_type=F32
            )
            lane_sq = lax.broadcasted_iota(jnp.int32, (LANES, LANES), 1)
            left = jnp.concatenate(
                [jnp.where(lane_sq % rows == b, columns, 0.0).astype(BF16) for b in range(rows)],
                axis=0,
            )
            high, low = halves(inkey)
            right = jnp.concatenate([high, low, high, none], axis=0)
            outer = jnp.dot(left, right, preferred_element_type=F32)
            reader = readkey.astype(BF16)
            fades = [
                jnp.broadcast_to(decay[:, k * head_dim : k * head_dim + 1], (rows, LANES))
                for k in range(heads)
            ]
            readout = jnp.zeros((rows, LANES), F32)
            for b in range(rows):
                news = []
                for k in range(heads):
                    at = (b * heads + k) * head_dim
                    new = fades[k][b : b + 1] * state_v[l, b, k] + outer[at : at + head_dim]
                    state_out[l, b, k] = new
                    news.append(new.astype(BF16))
                read = lax.dot_general(
                    reader,
                    jnp.concatenate(news, axis=0),
                    (((1,), (1,)), ((), ())),
                    preferred_element_type=F32,
                )
                readout = jnp.where(sub == b, read, readout)
            readout = readout + fixed_v[l, 3] * value
            gated = readout * jax.nn.silu(gate)
            scale = lax.rsqrt(jnp.mean(gated * gated, axis=1, keepdims=True) + EPSILON)
            normed = (gated * scale * out_gain[l : l + 1, :]).astype(BF16)
            if l + 1 < layers:
                wide_recv[me_quarter * n_dp + me_dp] = normed
            else:
                mix_recv[me_dp] = normed
            for r in range(roles):
                win_f[
                    l, pl.ds((r + 1) * width_back - 1, rows, stride=roles * width_back), :
                ] = current[r]

    def send_mix(l):
        if l + 1 < layers:
            here = wide_recv.at[me_quarter * n_dp + me_dp]
            for shift in dp_shifts:
                for near in range(1, blocks):
                    remote(here, here, mix_at(l), near_at(near) | dp_at(shift))
            for near in range(1, blocks):
                remote(here, here, mix_at(l), near_at(near))
        else:
            here = mix_recv.at[me_dp]
        for shift in dp_shifts:
            remote(here, here, mix_at(l), dp_at(shift))

    def wait_mix(l, sem):
        if l + 1 < layers:
            total_wait(wide_recv, blocks * n_dp - 1, sem)
        else:
            total_wait(mix_recv, n_dp - 1, sem)

    def send_weights():
        for near in range(1, blocks):
            quarter = lax.rem(me_quarter + near, blocks)
            columns = pl.ds(pl.multiple_of(quarter * LANES, LANES), LANES)
            remote(wo_v.at[0, :, columns], wo_near.at[me_quarter], weights_near, near_at(near))
        columns = pl.ds(pl.multiple_of(me_quarter * LANES, LANES), LANES)
        wo_near[me_quarter] = wo_v[0, :, columns]

    def reduce_all():
        with jax.named_scope("far_send"):
            mix = jnp.concatenate(
                [
                    jnp.concatenate(
                        [wide_recv[q * n_dp + i].astype(F32) for i in range(n_dp)], axis=0
                    ).astype(BF16)
                    for q in range(blocks)
                ],
                axis=1,
            )
            part = jnp.dot(
                mix, wo_near[...].reshape(-1, LANES), preferred_element_type=F32
            )
            pair_v[0] = part.astype(BF16)
            remote(pair_v.at[0], pair_v.at[1], pair_sum, {"tp": me_tp + blocks - 2 * blocks * odd})
            h = h_v[:, pl.ds(pl.multiple_of(me_quarter * LANES, LANES), LANES)].astype(F32)
        with jax.named_scope("pair_wait"):
            total_wait(pair_v, 1, recv_sem.at[pair_sum])
        with jax.named_scope("pair_send"):
            far_recv[me_pair] = (pair_v[0].astype(F32) + pair_v[1].astype(F32)).astype(BF16)
            pl.semaphore_wait(know_sem.at[1], 2)
            for step in range(far // 2, 0, -1):
                for shift in sorted({step, far - step}):
                    to = tp_at(shift * 2 * blocks)
                    remote(far_recv.at[me_pair], far_recv.at[me_pair], far_sum, to)
        with jax.named_scope("far_wait"):
            total_wait(far_recv, far - 1, recv_sem.at[far_sum])
        with jax.named_scope("near_all"):
            mine = (h + jnp.sum(far_recv[...].astype(F32), axis=0)).astype(BF16)
            own_recv[me_quarter] = mine
            for shift in range(1, blocks):
                remote(own_recv.at[me_quarter], own_recv.at[me_quarter], near_all, near_at(shift))
        with jax.named_scope("near_all_wait"):
            total_wait(own_recv, blocks - 1, recv_sem.at[near_all])
        return jnp.concatenate([own_recv[j].astype(F32) for j in range(blocks)], axis=1)

    def reduce_rows(l):
        with jax.named_scope("ring_send"):
            kept_rows = batch // n_tp
            mix = jnp.concatenate(
                [mix_recv[i].astype(F32) for i in range(n_dp)], axis=0
            ).astype(BF16)
            part = jnp.dot(mix, wo_v[l], preferred_element_type=F32)
            for j in range(blocks):
                tile_f[pl.ds(j, batch, stride=blocks), :] = part[:, j * LANES : (j + 1) * LANES]
            for i in range(n_tp):
                part_send[i] = tile_f[i * 8 : (i + 1) * 8, :].astype(BF16)

            def to(shift):
                at = lax.rem(me_tp + shift, n_tp)
                remote(part_send.at[at], part_recv.at[me_tp], ring_sum, {"tp": at})

            def pair(step, _):
                to(n_tp // 2 - step)
                to(n_tp // 2 + step)
                return 0

            to(n_tp // 2)
            lax.fori_loop(1, n_tp // 2, pair, 0)
            part_recv[me_tp] = part_send[me_tp]
        with jax.named_scope("ring_wait"):
            at_row = lax.broadcasted_iota(jnp.int32, (8, batch), 0)
            at_col = lax.broadcasted_iota(jnp.int32, (8, batch), 1)
            pick = ((at_col == kept_rows * me_tp + at_row) & (at_row < kept_rows)).astype(BF16)
            h = jnp.concatenate([own_recv[j] for j in range(blocks)], axis=1)
            kept = jnp.dot(pick, h, preferred_element_type=F32)[0:kept_rows]
            window(l)
            total_wait(part_recv, n_tp - 1, recv_sem.at[ring_sum])
        with jax.named_scope("ring_sum"):
            tile_f[0:8, :] = jnp.sum(part_recv[...].astype(F32), axis=0)
            update = jnp.concatenate(
                [tile_f[pl.ds(j, kept_rows, stride=blocks), :] for j in range(blocks)], axis=1
            )
            hidden_out[...] = (kept + update).astype(BF16)

    with jax.named_scope("load_wait"):
        for copy in h_load:
            copy.wait()
    project(0, h_v[...].astype(F32))
    with jax.named_scope("barrier"):
        pl.semaphore_wait(barrier, n_dp - 1 + 2 * blocks)
    with jax.named_scope("send_in0"):
        send_in(0)
        for to in (blocks, -blocks):
            signal(know_sem.at[0], tp_at(to))
        small_loads = [
            load(source, target, 2 + layers)
            for source, target in (
                (history, hist_v),
                (counts_in, counts),
                (taps_in, taps),
                (step_bias_in, step_bias),
                (decay_log_in, decay_log),
                (direct_gain_in, direct_gain),
                (extra_log_in, extra_log),
                (out_gain_in, out_gain),
            )
        ]
        state_loads = [load(state_in.at[0], state_v.at[0], 3 + layers)]
        wo_loads = [load(w_out.at[0], wo_v.at[0], 3 + 2 * layers)]
        for l in range(1, layers):
            w_loads.append(load_products(l))
            state_loads.append(load(state_in.at[l], state_v.at[l], 3 + layers + l))
            wo_loads.append(load(w_out.at[l], wo_v.at[l], 3 + 2 * layers + l))
        for copy in small_loads:
            copy.wait()
        for l in range(layers):
            earlier(l)
        wo_loads[0].wait()
        send_weights()
        state_loads[0].wait()

    for l in range(layers):
        with jax.named_scope(f"in_wait{l}"):
            total_wait(in_recv.at[l], n_dp - 1, recv_sem.at[in_at(l)])
        mixer(l)
        with jax.named_scope(f"send_mix{l}"):
            send_mix(l)
            if l == 0:
                pl.semaphore_wait(know_sem.at[0], 2)
                for to in (2 * blocks, -2 * blocks):
                    signal(know_sem.at[1], tp_at(to))
                window(l)
                total_wait(wo_near, blocks - 1, recv_sem.at[weights_near])
                for copy in w_loads[1]:
                    copy.wait()
        with jax.named_scope(f"mix_wait{l}"):
            wait_mix(l, recv_sem.at[mix_at(l)])
        if l + 1 < layers:
            project(l + 1, reduce_all())
            with jax.named_scope(f"send_in{l + 1}"):
                send_in(l + 1)
                state_loads[l + 1].wait()
                wo_loads[l + 1].wait()
        else:
            reduce_rows(l)

    with jax.named_scope("end"):
        for l in range(layers):
            total_wait(in_send.at[l], n_dp - 1, send_sem.at[in_at(l)])
            wait_mix(l, send_sem.at[mix_at(l)])
        total_wait(wo_near, blocks - 1, send_sem.at[weights_near])
        total_wait(far_recv, far - 1, send_sem.at[far_sum])
        total_wait(pair_v, 1, send_sem.at[pair_sum])
        total_wait(own_recv, blocks - 1, send_sem.at[near_all])
        total_wait(part_send, n_tp - 1, send_sem.at[ring_sum])


def write_out(pieces, hidden_v, states_v, windows_v, hidden, states, windows, sem):
    copies = [
        pltpu.make_async_copy(hidden_v, hidden, sem.at[0]),
        pltpu.make_async_copy(windows_v, windows, sem.at[1]),
    ]
    layers, batch = states.shape[:2]
    step = layers * batch // pieces
    for p in range(pieces):
        l, b = divmod(p * step, batch)
        part = pl.ds(b, step)
        copies.append(
            pltpu.make_async_copy(states_v.at[l, part], states.at[l, part], sem.at[2 + p])
        )
    for copy in copies:
        copy.start()
    for copy in copies:
        copy.wait()


def body(n_tp, n_dp, *args):
    args = list(args)
    args[7] = jnp.transpose(args[7], (0, 2, 1))
    args[8] = jnp.transpose(args[8], (1, 2, 0, 3))
    args[9] = jnp.transpose(args[9], (0, 1, 3, 2, 4))
    args[13] = jnp.transpose(args[13], (0, 2, 1))
    h, w_value, history, state, w_out = (args[k] for k in (0, 3, 9, 14, 16))
    layers, feats, chans = w_value.shape
    batch = h.shape[0]
    rows = batch // n_dp
    roles, width_back = history.shape[2:4]
    blocks = feats // LANES
    vmem = pl.BlockSpec(memory_space=pltpu.VMEM)
    hbm = pl.BlockSpec(memory_space=pl.ANY)
    kept = pltpu.VMEM((batch // n_tp, feats), BF16), pltpu.VMEM(state.shape, F32), pltpu.VMEM(
        history.shape, BF16
    )
    in_vmem = pl.pallas_call(
        functools.partial(kernel, n_tp, n_dp),
        out_shape=kept,
        in_specs=[hbm] * len(args),
        out_specs=(vmem, vmem, vmem),
        scratch_shapes=[
            pltpu.SMEM(args[1].shape, args[1].dtype),
            *(pltpu.VMEM(args[k].shape, args[k].dtype) for k in (2, 7, 8)),
            *(pltpu.SMEM(args[k].shape, args[k].dtype) for k in (10, 11, 12)),
            *(pltpu.VMEM(args[k].shape, args[k].dtype) for k in (13, 15)),
            pltpu.VMEM((batch, feats), BF16),
            pltpu.VMEM((layers, feats, 4 * chans), BF16),
            pltpu.VMEM(w_out.shape, BF16),
            pltpu.VMEM(history.shape, BF16),
            pltpu.VMEM(state.shape, F32),
            pltpu.VMEM((rows * roles * width_back, LANES), F32),
            pltpu.VMEM((layers, rows * roles * width_back, LANES), F32),
            pltpu.VMEM((layers, roles, rows, LANES), F32),
            pltpu.VMEM((layers, 4, rows, LANES), F32),
            pltpu.VMEM((n_tp * 8, LANES), F32),
            pltpu.VMEM((layers, n_dp, 5, rows, LANES), BF16),
            pltpu.VMEM((layers, n_dp, 5, rows, LANES), BF16),
            pltpu.VMEM((n_dp, rows, LANES), BF16),
            pltpu.VMEM((blocks * n_dp, rows, LANES), BF16),
            pltpu.VMEM((blocks, chans, LANES), BF16),
            pltpu.VMEM((2, batch, LANES), BF16),
            pltpu.VMEM((n_tp // (2 * blocks), batch, LANES), BF16),
            pltpu.VMEM((blocks, batch, LANES), BF16),
            pltpu.VMEM((n_tp, 8, LANES), BF16),
            pltpu.VMEM((n_tp, 8, LANES), BF16),
            pltpu.SemaphoreType.DMA((3 + 3 * layers,)),
            pltpu.SemaphoreType.DMA((2 * layers + 5,)),
            pltpu.SemaphoreType.DMA((2 * layers + 5,)),
            pltpu.SemaphoreType.REGULAR((2,)),
        ],
        compiler_params=pltpu.CompilerParams(collective_id=0, has_side_effects=True),
    )(*args)
    pieces = 4
    hidden, states, windows = pl.pallas_call(
        functools.partial(write_out, pieces),
        out_shape=tuple(jax.ShapeDtypeStruct(k.shape, k.dtype) for k in in_vmem),
        in_specs=[vmem] * 3,
        out_specs=(hbm, hbm, hbm),
        scratch_shapes=[pltpu.SemaphoreType.DMA((2 + pieces,))],
    )(*(pltpu.with_memory_space_constraint(k, pltpu.VMEM) for k in in_vmem))
    return hidden, states, jnp.transpose(windows, (0, 1, 3, 2, 4))


def solution(mesh):
    placed = (
        P("grp", "dp"),
        P(("grp", "dp")),
        P(None, "dp"),
        P(None, "dp", "tp"),
        P(None, "dp", "tp"),
        P(None, "dp", "tp"),
        P(None, "dp", "tp"),
        P(None, "dp", None),
        P(None, None, None, "tp"),
        P(None, ("grp", "dp"), None, None, "tp"),
        P(None, "tp"),
        P(None, "tp"),
        P(None, "tp"),
        P(None, ("grp", "dp"), "tp"),
        P(None, ("grp", "dp"), "tp", None, None),
        P(None, "tp"),
        P(None, "tp", "dp"),
    )
    return jax.shard_map(
        functools.partial(body, mesh.shape["tp"], mesh.shape["dp"]),
        mesh=mesh,
        in_specs=placed,
        out_specs=(
            P(("grp", "tp"), "dp"),
            P(None, ("grp", "dp"), "tp", None, None),
            P(None, ("grp", "dp"), None, None, "tp"),
        ),
        check_vma=False,
    )
```

```python
import functools

import jax
import jax.numpy as jnp
from jax import lax
from jax.experimental import pallas as pl
from jax.experimental.pallas import tpu as pltpu
from jax.sharding import PartitionSpec as P

D = 4096
EPSILON = 1e-06
MESH = pl.DeviceIdType.MESH
F32 = jnp.float32
BF16 = jnp.bfloat16
LANES = 128
STAT = 3


def total_wait(buffer, count, sem):
    part = buffer.at[pl.ds(0, count)]
    pltpu.make_async_copy(part, part, sem).wait()


def kernel(
    n_tp,
    n_dp,
    h_in,
    counts_in,
    in_gain_in,
    w_value,
    w_inkey,
    w_readkey,
    w_gate,
    w_step_in,
    taps_in,
    history,
    step_bias_in,
    decay_log_in,
    direct_gain_in,
    extra_log_in,
    state_in,
    out_gain_in,
    w_out,
    hidden_out,
    state_out,
    window_out,
    counts,
    in_gain,
    w_step,
    taps,
    step_bias,
    decay_log,
    direct_gain,
    extra_log,
    out_gain,
    h_v,
    wp_v,
    wo_v,
    hist_v,
    state_v,
    hist_f,
    win_f,
    early_v,
    fixed_v,
    tile_f,
    in_send,
    in_recv,
    mix_recv,
    wide_recv,
    wo_near,
    pair_v,
    far_recv,
    own_recv,
    part_send,
    part_recv,
    load_sem,
    send_sem,
    recv_sem,
    know_sem,
):
    layers = w_out.shape[0]
    batch, feats = h_in.shape
    rows = batch // n_dp
    blocks = feats // LANES
    head_dim = state_in.shape[3]
    heads = state_in.shape[2]
    roles, width_back = history.shape[2:4]
    far = n_tp // (2 * blocks)
    me_tp = lax.axis_index("tp")
    me_dp = lax.axis_index("dp")
    me_block = me_tp // blocks
    me_quarter = lax.rem(me_tp, blocks)
    me_pair = me_block // 2
    odd = lax.rem(me_block, 2)

    def tp_at(shift):
        return {"tp": lax.rem(me_tp + (n_tp + shift), n_tp)}

    def dp_at(shift):
        return {"dp": lax.rem(me_dp + shift, n_dp)}

    def near_at(shift):
        return {"tp": me_block * blocks + lax.rem(me_quarter + shift, blocks)}

    def remote(source, target, sem, to):
        pltpu.make_async_remote_copy(
            src_ref=source,
            dst_ref=target,
            send_sem=send_sem.at[sem],
            recv_sem=recv_sem.at[sem],
            device_id=to,
            device_id_type=MESH,
        ).start()

    def signal(sem, to):
        pl.semaphore_signal(sem, inc=1, device_id=to, device_id_type=MESH)

    in_at = lambda l: l
    mix_at = lambda l: layers + l
    weights_near, far_sum, near_all, ring_sum, pair_sum = (2 * layers + k for k in range(5))
    dp_shifts = sorted(range(1, n_dp), key=lambda s: abs(s - n_dp // 2))

    def load(source, target, sem):
        copy = pltpu.make_async_copy(source, target, load_sem.at[sem])
        copy.start()
        return copy

    def load_products(l):
        return [
            load(w.at[l], wp_v.at[l, :, pl.ds(k * LANES, LANES)], 1 + l)
            for k, w in enumerate((w_value, w_inkey, w_readkey, w_gate))
        ]

    h_load = [load(h_in, h_v, 0), load(in_gain_in, in_gain, 0)]
    w_loads = [load_products(0)]
    step_load = load(w_step_in, w_step, 1 + layers)

    barrier = pltpu.get_barrier_semaphore()
    for shift in range(1, n_dp):
        signal(barrier, dp_at(shift))
    for shift in range(1, blocks + 1):
        for to in (shift, -shift):
            signal(barrier, tp_at(to))

    lane = lax.broadcasted_iota(jnp.int32, (rows, LANES), 1)
    lane_all = lax.broadcasted_iota(jnp.int32, (batch, LANES), 1)
    sub = lax.broadcasted_iota(jnp.int32, (rows, LANES), 0)
    first_head = lane < head_dim
    unit = (
        lax.broadcasted_iota(jnp.int32, (LANES, LANES), 0)
        == lax.broadcasted_iota(jnp.int32, (LANES, LANES), 1)
    ).astype(BF16)

    def halves(x):
        high = x.astype(BF16)
        return high, (x - high.astype(F32)).astype(BF16)

    def spread(values, in_layer):
        return jnp.where(first_head, values[in_layer, 0], values[in_layer, 1])

    def project(l, h):
        with jax.named_scope(f"proj{l}"):
            squares = jnp.sum(h * h, axis=1, keepdims=True)
            scaled = (h * in_gain[l : l + 1, :]).astype(BF16)
            if l == 0:
                step_load.wait()
            steps = lax.dot_general(
                scaled, w_step[l], (((1,), (1,)), ((), ())), preferred_element_type=F32
            )
            lane_step = lax.broadcasted_iota(jnp.int32, steps.shape, 1)
            wanted = [
                jnp.sum(
                    jnp.where(lane_step == me_tp * heads + k, steps, 0.0), axis=1, keepdims=True
                )
                for k in range(heads)
            ] + [squares]
            if l == 0:
                for copy in w_loads[l]:
                    copy.wait()
            part = jnp.dot(scaled, wp_v[l], preferred_element_type=F32)
            stats = jnp.zeros((batch, LANES), F32)
            for k, v in enumerate(wanted):
                high = v.astype(BF16).astype(F32)
                stats = jnp.where(lane_all == k, high, stats)
                stats = jnp.where(lane_all == k + STAT, v - high, stats)
            for i in range(n_dp):
                at = slice(i * rows, (i + 1) * rows)
                for k in range(4):
                    in_send[l, i, k] = part[at, k * LANES : (k + 1) * LANES].astype(BF16)
                in_send[l, i, 4] = stats[at].astype(BF16)

    def send_in(l):
        for shift in dp_shifts:
            to = dp_at(shift)
            remote(in_send.at[l, to["dp"]], in_recv.at[l, me_dp], in_at(l), to)
        in_recv[l, me_dp] = in_send[l, me_dp]

    def earlier(l):
        lens = jnp.zeros((rows, LANES), jnp.int32)
        for b in range(rows):
            lens = jnp.where(sub == b, counts[b], lens)
        for b in range(rows):
            for r in range(roles):
                hist_f[pl.ds((b * roles + r) * width_back, width_back), :] = hist_v[
                    l, b, r
                ].astype(F32)
        for r in range(roles):
            total = jnp.zeros((rows, LANES), F32)
            for j in range(width_back):
                past = hist_f[pl.ds(r * width_back + j, rows, stride=roles * width_back), :]
                live = jnp.where(lens >= width_back - j, past, 0.0)
                total = total + live * taps[j, r, l : l + 1].astype(F32)
                if j:
                    win_f[
                        l, pl.ds(r * width_back + j - 1, rows, stride=roles * width_back), :
                    ] = past
            early_v[l, r] = total
        diagonal = lax.broadcasted_iota(jnp.int32, (rows, rows), 0) == lax.broadcasted_iota(
            jnp.int32, (rows, rows), 1
        )
        extra = [
            jnp.sum(jnp.where(diagonal, extra_log[l, k : k + 1, :], 0.0), axis=1, keepdims=True)
            for k in range(heads)
        ]
        fixed_v[l, 0] = jnp.where(first_head, extra[0], extra[1])
        fixed_v[l, 1] = jnp.exp(spread(decay_log, l))
        fixed_v[l, 2] = spread(step_bias, l)
        fixed_v[l, 3] = spread(direct_gain, l)

    def window(l):
        for b in range(rows):
            for r in range(roles):
                window_out[l, b, r] = win_f[
                    l, pl.ds((b * roles + r) * width_back, width_back), :
                ].astype(BF16)

    def mixer(l):
        with jax.named_scope(f"mixer{l}"):
            arrived = jnp.sum(in_recv[l].astype(F32), axis=0)
            stats = arrived[4]

            def stat(k):
                both = jnp.where((lane == k) | (lane == k + STAT), stats, 0.0)
                return jnp.sum(both, axis=1, keepdims=True)

            inverse = lax.rsqrt(stat(heads) / D + EPSILON)
            current = [(inverse * arrived[k]).astype(BF16).astype(F32) for k in range(roles)]
            gate = (inverse * arrived[3]).astype(BF16).astype(F32)
            step = jnp.where(first_head, stat(0), stat(1)) * inverse
            step = step.astype(BF16).astype(F32)
            value, inkey, readkey = [
                jax.nn.silu(
                    early_v[l, r] + current[r] * taps[width_back, r, l : l + 1].astype(F32)
                )
                for r in range(roles)
            ]
            rate = jax.nn.softplus(step + fixed_v[l, 2])
            decay = jnp.exp(-rate * fixed_v[l, 1] + fixed_v[l, 0])
            gain = rate * value
            high, low = halves(gain)
            none = jnp.zeros((LANES - 3 * rows, LANES), BF16)
            parts = jnp.concatenate([high, high, low, none], axis=0)
            columns = lax.dot_general(
                unit, parts, (((1,), (1,)), ((), ())), preferred_element_type=F32
            )
            lane_sq = lax.broadcasted_iota(jnp.int32, (LANES, LANES), 1)
            left = jnp.concatenate(
                [jnp.where(lane_sq % rows == b, columns, 0.0).astype(BF16) for b in range(rows)],
                axis=0,
            )
            high, low = halves(inkey)
            right = jnp.concatenate([high, low, high, none], axis=0)
            outer = jnp.dot(left, right, preferred_element_type=F32)
            reader = readkey.astype(BF16)
            fades = [
                jnp.broadcast_to(decay[:, k * head_dim : k * head_dim + 1], (rows, LANES))
                for k in range(heads)
            ]
            readout = jnp.zeros((rows, LANES), F32)
            for b in range(rows):
                news = []
                for k in range(heads):
                    at = (b * heads + k) * head_dim
                    new = fades[k][b : b + 1] * state_v[l, b, k] + outer[at : at + head_dim]
                    state_out[l, b, k] = new
                    news.append(new.astype(BF16))
                read = lax.dot_general(
                    reader,
                    jnp.concatenate(news, axis=0),
                    (((1,), (1,)), ((), ())),
                    preferred_element_type=F32,
                )
                readout = jnp.where(sub == b, read, readout)
            readout = readout + fixed_v[l, 3] * value
            gated = readout * jax.nn.silu(gate)
            scale = lax.rsqrt(jnp.mean(gated * gated, axis=1, keepdims=True) + EPSILON)
            normed = (gated * scale * out_gain[l : l + 1, :]).astype(BF16)
            if l + 1 < layers:
                wide_recv[me_quarter * n_dp + me_dp] = normed
            else:
                mix_recv[me_dp] = normed
            for r in range(roles):
                win_f[
                    l, pl.ds((r + 1) * width_back - 1, rows, stride=roles * width_back), :
                ] = current[r]

    def send_mix(l):
        if l + 1 < layers:
            here = wide_recv.at[me_quarter * n_dp + me_dp]
            for shift in dp_shifts:
                for near in range(1, blocks):
                    remote(here, here, mix_at(l), near_at(near) | dp_at(shift))
            for near in range(1, blocks):
                remote(here, here, mix_at(l), near_at(near))
        else:
            here = mix_recv.at[me_dp]
        for shift in dp_shifts:
            remote(here, here, mix_at(l), dp_at(shift))

    def wait_mix(l, sem):
        if l + 1 < layers:
            total_wait(wide_recv, blocks * n_dp - 1, sem)
        else:
            total_wait(mix_recv, n_dp - 1, sem)

    def send_weights():
        for near in range(1, blocks):
            quarter = lax.rem(me_quarter + near, blocks)
            columns = pl.ds(pl.multiple_of(quarter * LANES, LANES), LANES)
            remote(wo_v.at[0, :, columns], wo_near.at[me_quarter], weights_near, near_at(near))
        columns = pl.ds(pl.multiple_of(me_quarter * LANES, LANES), LANES)
        wo_near[me_quarter] = wo_v[0, :, columns]

    def reduce_all():
        with jax.named_scope("far_send"):
            mix = jnp.concatenate(
                [
                    jnp.concatenate(
                        [wide_recv[q * n_dp + i].astype(F32) for i in range(n_dp)], axis=0
                    ).astype(BF16)
                    for q in range(blocks)
                ],
                axis=1,
            )
            part = jnp.dot(
                mix, wo_near[...].reshape(-1, LANES), preferred_element_type=F32
            )
            pair_v[0] = part.astype(BF16)
            remote(pair_v.at[0], pair_v.at[1], pair_sum, {"tp": me_tp + blocks - 2 * blocks * odd})
            h = h_v[:, pl.ds(pl.multiple_of(me_quarter * LANES, LANES), LANES)].astype(F32)
        with jax.named_scope("pair_wait"):
            total_wait(pair_v, 1, recv_sem.at[pair_sum])
        with jax.named_scope("pair_send"):
            far_recv[me_pair] = (pair_v[0].astype(F32) + pair_v[1].astype(F32)).astype(BF16)
            pl.semaphore_wait(know_sem.at[1], 2)
            for step in range(far - 1, 0, -1):
                away = step * blocks * (2 * odd - 1)
                to = {"tp": lax.rem(me_tp + n_tp + away, n_tp)}
                remote(far_recv.at[me_pair], far_recv.at[me_pair], far_sum, to)
        with jax.named_scope("far_wait"):
            total_wait(far_recv, far - 1, recv_sem.at[far_sum])
        with jax.named_scope("near_all"):
            mine = (h + jnp.sum(far_recv[...].astype(F32), axis=0)).astype(BF16)
            own_recv[me_quarter] = mine
            for shift in range(1, blocks):
                remote(own_recv.at[me_quarter], own_recv.at[me_quarter], near_all, near_at(shift))
        with jax.named_scope("near_all_wait"):
            total_wait(own_recv, blocks - 1, recv_sem.at[near_all])
        return jnp.concatenate([own_recv[j].astype(F32) for j in range(blocks)], axis=1)

    def reduce_rows(l):
        with jax.named_scope("ring_send"):
            kept_rows = batch // n_tp
            mix = jnp.concatenate(
                [mix_recv[i].astype(F32) for i in range(n_dp)], axis=0
            ).astype(BF16)
            part = jnp.dot(mix, wo_v[l], preferred_element_type=F32)
            for j in range(blocks):
                tile_f[pl.ds(j, batch, stride=blocks), :] = part[:, j * LANES : (j + 1) * LANES]
            for i in range(n_tp):
                part_send[i] = tile_f[i * 8 : (i + 1) * 8, :].astype(BF16)

            def to(shift):
                at = lax.rem(me_tp + shift, n_tp)
                remote(part_send.at[at], part_recv.at[me_tp], ring_sum, {"tp": at})

            def pair(step, _):
                to(n_tp // 2 - step)
                to(n_tp // 2 + step)
                return 0

            to(n_tp // 2)
            lax.fori_loop(1, n_tp // 2, pair, 0)
            part_recv[me_tp] = part_send[me_tp]
        with jax.named_scope("ring_wait"):
            at_row = lax.broadcasted_iota(jnp.int32, (8, batch), 0)
            at_col = lax.broadcasted_iota(jnp.int32, (8, batch), 1)
            pick = ((at_col == kept_rows * me_tp + at_row) & (at_row < kept_rows)).astype(BF16)
            h = jnp.concatenate([own_recv[j] for j in range(blocks)], axis=1)
            kept = jnp.dot(pick, h, preferred_element_type=F32)[0:kept_rows]
            window(l)
            total_wait(part_recv, n_tp - 1, recv_sem.at[ring_sum])
        with jax.named_scope("ring_sum"):
            tile_f[0:8, :] = jnp.sum(part_recv[...].astype(F32), axis=0)
            update = jnp.concatenate(
                [tile_f[pl.ds(j, kept_rows, stride=blocks), :] for j in range(blocks)], axis=1
            )
            hidden_out[...] = (kept + update).astype(BF16)

    with jax.named_scope("load_wait"):
        for copy in h_load:
            copy.wait()
    project(0, h_v[...].astype(F32))
    with jax.named_scope("barrier"):
        pl.semaphore_wait(barrier, n_dp - 1 + 2 * blocks)
    with jax.named_scope("send_in0"):
        send_in(0)
        for to in (blocks, -blocks):
            signal(know_sem.at[0], tp_at(to))
        small_loads = [
            load(source, target, 2 + layers)
            for source, target in (
                (history, hist_v),
                (counts_in, counts),
                (taps_in, taps),
                (step_bias_in, step_bias),
                (decay_log_in, decay_log),
                (direct_gain_in, direct_gain),
                (extra_log_in, extra_log),
                (out_gain_in, out_gain),
            )
        ]
        state_loads = [load(state_in.at[0], state_v.at[0], 3 + layers)]
        wo_loads = [load(w_out.at[0], wo_v.at[0], 3 + 2 * layers)]
        for l in range(1, layers):
            w_loads.append(load_products(l))
            state_loads.append(load(state_in.at[l], state_v.at[l], 3 + layers + l))
            wo_loads.append(load(w_out.at[l], wo_v.at[l], 3 + 2 * layers + l))
        for copy in small_loads:
            copy.wait()
        for l in range(layers):
            earlier(l)
        wo_loads[0].wait()
        send_weights()
        state_loads[0].wait()

    for l in range(layers):
        with jax.named_scope(f"in_wait{l}"):
            total_wait(in_recv.at[l], n_dp - 1, recv_sem.at[in_at(l)])
        mixer(l)
        with jax.named_scope(f"send_mix{l}"):
            send_mix(l)
            if l == 0:
                pl.semaphore_wait(know_sem.at[0], 2)
                for to in (2 * blocks, -2 * blocks):
                    signal(know_sem.at[1], tp_at(to))
                window(l)
                total_wait(wo_near, blocks - 1, recv_sem.at[weights_near])
                for copy in w_loads[1]:
                    copy.wait()
        with jax.named_scope(f"mix_wait{l}"):
            wait_mix(l, recv_sem.at[mix_at(l)])
        if l + 1 < layers:
            project(l + 1, reduce_all())
            with jax.named_scope(f"send_in{l + 1}"):
                send_in(l + 1)
                state_loads[l + 1].wait()
                wo_loads[l + 1].wait()
        else:
            reduce_rows(l)

    with jax.named_scope("end"):
        for l in range(layers):
            total_wait(in_send.at[l], n_dp - 1, send_sem.at[in_at(l)])
            wait_mix(l, send_sem.at[mix_at(l)])
        total_wait(wo_near, blocks - 1, send_sem.at[weights_near])
        total_wait(far_recv, far - 1, send_sem.at[far_sum])
        total_wait(pair_v, 1, send_sem.at[pair_sum])
        total_wait(own_recv, blocks - 1, send_sem.at[near_all])
        total_wait(part_send, n_tp - 1, send_sem.at[ring_sum])


def write_out(pieces, hidden_v, states_v, windows_v, hidden, states, windows, sem):
    copies = [
        pltpu.make_async_copy(hidden_v, hidden, sem.at[0]),
        pltpu.make_async_copy(windows_v, windows, sem.at[1]),
    ]
    layers, batch = states.shape[:2]
    step = layers * batch // pieces
    for p in range(pieces):
        l, b = divmod(p * step, batch)
        part = pl.ds(b, step)
        copies.append(
            pltpu.make_async_copy(states_v.at[l, part], states.at[l, part], sem.at[2 + p])
        )
    for copy in copies:
        copy.start()
    for copy in copies:
        copy.wait()


def body(n_tp, n_dp, *args):
    args = list(args)
    args[7] = jnp.transpose(args[7], (0, 2, 1))
    args[8] = jnp.transpose(args[8], (1, 2, 0, 3))
    args[9] = jnp.transpose(args[9], (0, 1, 3, 2, 4))
    args[13] = jnp.transpose(args[13], (0, 2, 1))
    h, w_value, history, state, w_out = (args[k] for k in (0, 3, 9, 14, 16))
    layers, feats, chans = w_value.shape
    batch = h.shape[0]
    rows = batch // n_dp
    roles, width_back = history.shape[2:4]
    blocks = feats // LANES
    vmem = pl.BlockSpec(memory_space=pltpu.VMEM)
    hbm = pl.BlockSpec(memory_space=pl.ANY)
    kept = pltpu.VMEM((batch // n_tp, feats), BF16), pltpu.VMEM(state.shape, F32), pltpu.VMEM(
        history.shape, BF16
    )
    in_vmem = pl.pallas_call(
        functools.partial(kernel, n_tp, n_dp),
        out_shape=kept,
        in_specs=[hbm] * len(args),
        out_specs=(vmem, vmem, vmem),
        scratch_shapes=[
            pltpu.SMEM(args[1].shape, args[1].dtype),
            *(pltpu.VMEM(args[k].shape, args[k].dtype) for k in (2, 7, 8)),
            *(pltpu.SMEM(args[k].shape, args[k].dtype) for k in (10, 11, 12)),
            *(pltpu.VMEM(args[k].shape, args[k].dtype) for k in (13, 15)),
            pltpu.VMEM((batch, feats), BF16),
            pltpu.VMEM((layers, feats, 4 * chans), BF16),
            pltpu.VMEM(w_out.shape, BF16),
            pltpu.VMEM(history.shape, BF16),
            pltpu.VMEM(state.shape, F32),
            pltpu.VMEM((rows * roles * width_back, LANES), F32),
            pltpu.VMEM((layers, rows * roles * width_back, LANES), F32),
            pltpu.VMEM((layers, roles, rows, LANES), F32),
            pltpu.VMEM((layers, 4, rows, LANES), F32),
            pltpu.VMEM((n_tp * 8, LANES), F32),
            pltpu.VMEM((layers, n_dp, 5, rows, LANES), BF16),
            pltpu.VMEM((layers, n_dp, 5, rows, LANES), BF16),
            pltpu.VMEM((n_dp, rows, LANES), BF16),
            pltpu.VMEM((blocks * n_dp, rows, LANES), BF16),
            pltpu.VMEM((blocks, chans, LANES), BF16),
            pltpu.VMEM((2, batch, LANES), BF16),
            pltpu.VMEM((n_tp // (2 * blocks), batch, LANES), BF16),
            pltpu.VMEM((blocks, batch, LANES), BF16),
            pltpu.VMEM((n_tp, 8, LANES), BF16),
            pltpu.VMEM((n_tp, 8, LANES), BF16),
            pltpu.SemaphoreType.DMA((3 + 3 * layers,)),
            pltpu.SemaphoreType.DMA((2 * layers + 5,)),
            pltpu.SemaphoreType.DMA((2 * layers + 5,)),
            pltpu.SemaphoreType.REGULAR((2,)),
        ],
        compiler_params=pltpu.CompilerParams(collective_id=0, has_side_effects=True),
    )(*args)
    pieces = 4
    hidden, states, windows = pl.pallas_call(
        functools.partial(write_out, pieces),
        out_shape=tuple(jax.ShapeDtypeStruct(k.shape, k.dtype) for k in in_vmem),
        in_specs=[vmem] * 3,
        out_specs=(hbm, hbm, hbm),
        scratch_shapes=[pltpu.SemaphoreType.DMA((2 + pieces,))],
    )(*(pltpu.with_memory_space_constraint(k, pltpu.VMEM) for k in in_vmem))
    return hidden, states, jnp.transpose(windows, (0, 1, 3, 2, 4))


def solution(mesh):
    placed = (
        P("grp", "dp"),
        P(("grp", "dp")),
        P(None, "dp"),
        P(None, "dp", "tp"),
        P(None, "dp", "tp"),
        P(None, "dp", "tp"),
        P(None, "dp", "tp"),
        P(None, "dp", None),
        P(None, None, None, "tp"),
        P(None, ("grp", "dp"), None, None, "tp"),
        P(None, "tp"),
        P(None, "tp"),
        P(None, "tp"),
        P(None, ("grp", "dp"), "tp"),
        P(None, ("grp", "dp"), "tp", None, None),
        P(None, "tp"),
        P(None, "tp", "dp"),
    )
    return jax.shard_map(
        functools.partial(body, mesh.shape["tp"], mesh.shape["dp"]),
        mesh=mesh,
        in_specs=placed,
        out_specs=(
            P(("grp", "tp"), "dp"),
            P(None, ("grp", "dp"), "tp", None, None),
            P(None, ("grp", "dp"), None, None, "tp"),
        ),
        check_vma=False,
    )
```

```python
import functools

import jax
import jax.numpy as jnp
from jax import lax
from jax.experimental import pallas as pl
from jax.experimental.pallas import tpu as pltpu
from jax.sharding import PartitionSpec as P

D = 4096
EPSILON = 1e-06
MESH = pl.DeviceIdType.MESH
F32 = jnp.float32
BF16 = jnp.bfloat16
LANES = 128
STAT = 3
SPACING = 2000


def total_wait(buffer, count, sem):
    part = buffer.at[pl.ds(0, count)]
    pltpu.make_async_copy(part, part, sem).wait()


def kernel(
    n_tp,
    n_dp,
    h_in,
    counts_in,
    in_gain_in,
    w_value,
    w_inkey,
    w_readkey,
    w_gate,
    w_step_in,
    taps_in,
    history,
    step_bias_in,
    decay_log_in,
    direct_gain_in,
    extra_log_in,
    state_in,
    out_gain_in,
    w_out,
    hidden_out,
    state_out,
    window_out,
    counts,
    in_gain,
    w_step,
    taps,
    step_bias,
    decay_log,
    direct_gain,
    extra_log,
    out_gain,
    h_v,
    wp_v,
    wo_v,
    hist_v,
    state_v,
    hist_f,
    win_f,
    early_v,
    fixed_v,
    tile_f,
    in_send,
    in_recv,
    mix_recv,
    wide_recv,
    wo_near,
    pair_v,
    far_recv,
    own_recv,
    part_send,
    part_recv,
    load_sem,
    send_sem,
    recv_sem,
    know_sem,
):
    layers = w_out.shape[0]
    batch, feats = h_in.shape
    rows = batch // n_dp
    blocks = feats // LANES
    head_dim = state_in.shape[3]
    heads = state_in.shape[2]
    roles, width_back = history.shape[2:4]
    far = n_tp // (2 * blocks)
    me_tp = lax.axis_index("tp")
    me_dp = lax.axis_index("dp")
    me_block = me_tp // blocks
    me_quarter = lax.rem(me_tp, blocks)
    me_pair = me_block // 2
    odd = lax.rem(me_block, 2)

    def tp_at(shift):
        return {"tp": lax.rem(me_tp + (n_tp + shift), n_tp)}

    def dp_at(shift):
        return {"dp": lax.rem(me_dp + shift, n_dp)}

    near = [
        blocks - 1 - me_quarter,
        me_quarter + 2 - 4 * (me_quarter // 2),
        me_quarter + 1 - 2 * lax.rem(me_quarter, 2),
    ]
    assert blocks == len(near) + 1

    def near_at(quarter):
        return {"tp": me_block * blocks + quarter}

    def remote(source, target, sem, to):
        pltpu.make_async_remote_copy(
            src_ref=source,
            dst_ref=target,
            send_sem=send_sem.at[sem],
            recv_sem=recv_sem.at[sem],
            device_id=to,
            device_id_type=MESH,
        ).start()

    def signal(sem, to):
        pl.semaphore_signal(sem, inc=1, device_id=to, device_id_type=MESH)

    in_at = lambda l: l
    mix_at = lambda l: layers + l
    weights_near, far_sum, near_all, ring_sum, pair_sum = (2 * layers + k for k in range(5))
    dp_shifts = sorted(range(1, n_dp), key=lambda s: abs(s - n_dp // 2))

    def load(source, target, sem):
        copy = pltpu.make_async_copy(source, target, load_sem.at[sem])
        copy.start()
        return copy

    def load_products(l):
        return [
            load(w.at[l], wp_v.at[l, :, pl.ds(k * LANES, LANES)], 1 + l)
            for k, w in enumerate((w_value, w_inkey, w_readkey, w_gate))
        ]

    h_load = [load(h_in, h_v, 0), load(in_gain_in, in_gain, 0)]
    w_loads = [load_products(0)]
    step_load = load(w_step_in, w_step, 1 + layers)

    barrier = pltpu.get_barrier_semaphore()
    for shift in range(1, n_dp):
        signal(barrier, dp_at(shift))
    for shift in range(1, blocks + 1):
        for to in (shift, -shift):
            signal(barrier, tp_at(to))

    lane = lax.broadcasted_iota(jnp.int32, (rows, LANES), 1)
    lane_all = lax.broadcasted_iota(jnp.int32, (batch, LANES), 1)
    sub = lax.broadcasted_iota(jnp.int32, (rows, LANES), 0)
    first_head = lane < head_dim
    unit = (
        lax.broadcasted_iota(jnp.int32, (LANES, LANES), 0)
        == lax.broadcasted_iota(jnp.int32, (LANES, LANES), 1)
    ).astype(BF16)

    def halves(x):
        high = x.astype(BF16)
        return high, (x - high.astype(F32)).astype(BF16)

    def spread(values, in_layer):
        return jnp.where(first_head, values[in_layer, 0], values[in_layer, 1])

    def project(l, h):
        with jax.named_scope(f"proj{l}"):
            squares = jnp.sum(h * h, axis=1, keepdims=True)
            scaled = (h * in_gain[l : l + 1, :]).astype(BF16)
            if l == 0:
                step_load.wait()
            steps = lax.dot_general(
                scaled, w_step[l], (((1,), (1,)), ((), ())), preferred_element_type=F32
            )
            lane_step = lax.broadcasted_iota(jnp.int32, steps.shape, 1)
            wanted = [
                jnp.sum(
                    jnp.where(lane_step == me_tp * heads + k, steps, 0.0), axis=1, keepdims=True
                )
                for k in range(heads)
            ] + [squares]
            if l == 0:
                for copy in w_loads[l]:
                    copy.wait()
            part = jnp.dot(scaled, wp_v[l], preferred_element_type=F32)
            stats = jnp.zeros((batch, LANES), F32)
            for k, v in enumerate(wanted):
                high = v.astype(BF16).astype(F32)
                stats = jnp.where(lane_all == k, high, stats)
                stats = jnp.where(lane_all == k + STAT, v - high, stats)
            for i in range(n_dp):
                at = slice(i * rows, (i + 1) * rows)
                for k in range(4):
                    in_send[l, i, k] = part[at, k * LANES : (k + 1) * LANES].astype(BF16)
                in_send[l, i, 4] = stats[at].astype(BF16)

    def send_in(l):
        for shift in dp_shifts:
            to = dp_at(shift)
            remote(in_send.at[l, to["dp"]], in_recv.at[l, me_dp], in_at(l), to)
        in_recv[l, me_dp] = in_send[l, me_dp]

    def earlier(l):
        lens = jnp.zeros((rows, LANES), jnp.int32)
        for b in range(rows):
            lens = jnp.where(sub == b, counts[b], lens)
        for b in range(rows):
            for r in range(roles):
                hist_f[pl.ds((b * roles + r) * width_back, width_back), :] = hist_v[
                    l, b, r
                ].astype(F32)
        for r in range(roles):
            total = jnp.zeros((rows, LANES), F32)
            for j in range(width_back):
                past = hist_f[pl.ds(r * width_back + j, rows, stride=roles * width_back), :]
                live = jnp.where(lens >= width_back - j, past, 0.0)
                total = total + live * taps[j, r, l : l + 1].astype(F32)
                if j:
                    win_f[
                        l, pl.ds(r * width_back + j - 1, rows, stride=roles * width_back), :
                    ] = past
            early_v[l, r] = total
        diagonal = lax.broadcasted_iota(jnp.int32, (rows, rows), 0) == lax.broadcasted_iota(
            jnp.int32, (rows, rows), 1
        )
        extra = [
            jnp.sum(jnp.where(diagonal, extra_log[l, k : k + 1, :], 0.0), axis=1, keepdims=True)
            for k in range(heads)
        ]
        fixed_v[l, 0] = jnp.where(first_head, extra[0], extra[1])
        fixed_v[l, 1] = jnp.exp(spread(decay_log, l))
        fixed_v[l, 2] = spread(step_bias, l)
        fixed_v[l, 3] = spread(direct_gain, l)

    def window(l):
        for b in range(rows):
            for r in range(roles):
                window_out[l, b, r] = win_f[
                    l, pl.ds((b * roles + r) * width_back, width_back), :
                ].astype(BF16)

    def mixer(l):
        with jax.named_scope(f"mixer{l}"):
            arrived = jnp.sum(in_recv[l].astype(F32), axis=0)
            stats = arrived[4]

            def stat(k):
                both = jnp.where((lane == k) | (lane == k + STAT), stats, 0.0)
                return jnp.sum(both, axis=1, keepdims=True)

            inverse = lax.rsqrt(stat(heads) / D + EPSILON)
            current = [(inverse * arrived[k]).astype(BF16).astype(F32) for k in range(roles)]
            gate = (inverse * arrived[3]).astype(BF16).astype(F32)
            step = jnp.where(first_head, stat(0), stat(1)) * inverse
            step = step.astype(BF16).astype(F32)
            value, inkey, readkey = [
                jax.nn.silu(
                    early_v[l, r] + current[r] * taps[width_back, r, l : l + 1].astype(F32)
                )
                for r in range(roles)
            ]
            rate = jax.nn.softplus(step + fixed_v[l, 2])
            decay = jnp.exp(-rate * fixed_v[l, 1] + fixed_v[l, 0])
            gain = rate * value
            high, low = halves(gain)
            none = jnp.zeros((LANES - 3 * rows, LANES), BF16)
            parts = jnp.concatenate([high, high, low, none], axis=0)
            columns = lax.dot_general(
                unit, parts, (((1,), (1,)), ((), ())), preferred_element_type=F32
            )
            lane_sq = lax.broadcasted_iota(jnp.int32, (LANES, LANES), 1)
            left = jnp.concatenate(
                [jnp.where(lane_sq % rows == b, columns, 0.0).astype(BF16) for b in range(rows)],
                axis=0,
            )
            high, low = halves(inkey)
            right = jnp.concatenate([high, low, high, none], axis=0)
            outer = jnp.dot(left, right, preferred_element_type=F32)
            reader = readkey.astype(BF16)
            fades = [
                jnp.broadcast_to(decay[:, k * head_dim : k * head_dim + 1], (rows, LANES))
                for k in range(heads)
            ]
            readout = jnp.zeros((rows, LANES), F32)
            for b in range(rows):
                news = []
                for k in range(heads):
                    at = (b * heads + k) * head_dim
                    new = fades[k][b : b + 1] * state_v[l, b, k] + outer[at : at + head_dim]
                    state_out[l, b, k] = new
                    news.append(new.astype(BF16))
                read = lax.dot_general(
                    reader,
                    jnp.concatenate(news, axis=0),
                    (((1,), (1,)), ((), ())),
                    preferred_element_type=F32,
                )
                readout = jnp.where(sub == b, read, readout)
            readout = readout + fixed_v[l, 3] * value
            gated = readout * jax.nn.silu(gate)
            scale = lax.rsqrt(jnp.mean(gated * gated, axis=1, keepdims=True) + EPSILON)
            normed = (gated * scale * out_gain[l : l + 1, :]).astype(BF16)
            if l + 1 < layers:
                wide_recv[me_quarter * n_dp + me_dp] = normed
            else:
                mix_recv[me_dp] = normed
            for r in range(roles):
                win_f[
                    l, pl.ds((r + 1) * width_back - 1, rows, stride=roles * width_back), :
                ] = current[r]

    def send_mix(l):
        if l + 1 < layers:
            here = wide_recv.at[me_quarter * n_dp + me_dp]
            for shift in dp_shifts:
                for quarter in near:
                    remote(here, here, mix_at(l), near_at(quarter) | dp_at(shift))
            for quarter in near:
                remote(here, here, mix_at(l), near_at(quarter))
        else:
            here = mix_recv.at[me_dp]
        for shift in dp_shifts:
            remote(here, here, mix_at(l), dp_at(shift))

    def wait_mix(l, sem):
        if l + 1 < layers:
            total_wait(wide_recv, blocks * n_dp - 1, sem)
        else:
            total_wait(mix_recv, n_dp - 1, sem)

    def send_weights():
        for quarter in near:
            columns = pl.ds(pl.multiple_of(quarter * LANES, LANES), LANES)
            remote(wo_v.at[0, :, columns], wo_near.at[me_quarter], weights_near, near_at(quarter))
        columns = pl.ds(pl.multiple_of(me_quarter * LANES, LANES), LANES)
        wo_near[me_quarter] = wo_v[0, :, columns]

    def reduce_all():
        with jax.named_scope("far_send"):
            mix = jnp.concatenate(
                [
                    jnp.concatenate(
                        [wide_recv[q * n_dp + i].astype(F32) for i in range(n_dp)], axis=0
                    ).astype(BF16)
                    for q in range(blocks)
                ],
                axis=1,
            )
            part = jnp.dot(
                mix, wo_near[...].reshape(-1, LANES), preferred_element_type=F32
            )
            pair_v[0] = part.astype(BF16)
            remote(pair_v.at[0], pair_v.at[1], pair_sum, {"tp": me_tp + blocks - 2 * blocks * odd})
            h = h_v[:, pl.ds(pl.multiple_of(me_quarter * LANES, LANES), LANES)].astype(F32)
        with jax.named_scope("pair_wait"):
            total_wait(pair_v, 1, recv_sem.at[pair_sum])
        with jax.named_scope("pair_send"):
            far_recv[me_pair] = (pair_v[0].astype(F32) + pair_v[1].astype(F32)).astype(BF16)
            pl.semaphore_wait(know_sem.at[1], 2)
            for step in range(far - 1, 0, -1):
                if step < far - 1:
                    pl.delay(SPACING)
                away = step * blocks * (2 * odd - 1)
                to = {"tp": lax.rem(me_tp + n_tp + away, n_tp)}
                remote(far_recv.at[me_pair], far_recv.at[me_pair], far_sum, to)
        with jax.named_scope("far_wait"):
            total_wait(far_recv, far - 1, recv_sem.at[far_sum])
        with jax.named_scope("near_all"):
            mine = (h + jnp.sum(far_recv[...].astype(F32), axis=0)).astype(BF16)
            own_recv[me_quarter] = mine
            for quarter in near:
                remote(own_recv.at[me_quarter], own_recv.at[me_quarter], near_all, near_at(quarter))
        with jax.named_scope("near_all_wait"):
            total_wait(own_recv, blocks - 1, recv_sem.at[near_all])
        return jnp.concatenate([own_recv[j].astype(F32) for j in range(blocks)], axis=1)

    def reduce_rows(l):
        with jax.named_scope("ring_send"):
            kept_rows = batch // n_tp
            mix = jnp.concatenate(
                [mix_recv[i].astype(F32) for i in range(n_dp)], axis=0
            ).astype(BF16)
            part = jnp.dot(mix, wo_v[l], preferred_element_type=F32)
            for j in range(blocks):
                tile_f[pl.ds(j, batch, stride=blocks), :] = part[:, j * LANES : (j + 1) * LANES]
            for i in range(n_tp):
                part_send[i] = tile_f[i * 8 : (i + 1) * 8, :].astype(BF16)

            def to(shift):
                at = lax.rem(me_tp + shift, n_tp)
                remote(part_send.at[at], part_recv.at[me_tp], ring_sum, {"tp": at})

            def pair(step, _):
                to(n_tp // 2 - step)
                to(n_tp // 2 + step)
                return 0

            to(n_tp // 2)
            lax.fori_loop(1, n_tp // 2, pair, 0)
            part_recv[me_tp] = part_send[me_tp]
        with jax.named_scope("ring_wait"):
            at_row = lax.broadcasted_iota(jnp.int32, (8, batch), 0)
            at_col = lax.broadcasted_iota(jnp.int32, (8, batch), 1)
            pick = ((at_col == kept_rows * me_tp + at_row) & (at_row < kept_rows)).astype(BF16)
            h = jnp.concatenate([own_recv[j] for j in range(blocks)], axis=1)
            kept = jnp.dot(pick, h, preferred_element_type=F32)[0:kept_rows]
            window(l)
            total_wait(part_recv, n_tp - 1, recv_sem.at[ring_sum])
        with jax.named_scope("ring_sum"):
            tile_f[0:8, :] = jnp.sum(part_recv[...].astype(F32), axis=0)
            update = jnp.concatenate(
                [tile_f[pl.ds(j, kept_rows, stride=blocks), :] for j in range(blocks)], axis=1
            )
            hidden_out[...] = (kept + update).astype(BF16)

    with jax.named_scope("load_wait"):
        for copy in h_load:
            copy.wait()
    project(0, h_v[...].astype(F32))
    with jax.named_scope("barrier"):
        pl.semaphore_wait(barrier, n_dp - 1 + 2 * blocks)
    with jax.named_scope("send_in0"):
        send_in(0)
        for to in (blocks, -blocks):
            signal(know_sem.at[0], tp_at(to))
        small_loads = [
            load(source, target, 2 + layers)
            for source, target in (
                (history, hist_v),
                (counts_in, counts),
                (taps_in, taps),
                (step_bias_in, step_bias),
                (decay_log_in, decay_log),
                (direct_gain_in, direct_gain),
                (extra_log_in, extra_log),
                (out_gain_in, out_gain),
            )
        ]
        state_loads = [load(state_in.at[0], state_v.at[0], 3 + layers)]
        wo_loads = [load(w_out.at[0], wo_v.at[0], 3 + 2 * layers)]
        for l in range(1, layers):
            w_loads.append(load_products(l))
            state_loads.append(load(state_in.at[l], state_v.at[l], 3 + layers + l))
            wo_loads.append(load(w_out.at[l], wo_v.at[l], 3 + 2 * layers + l))
        for copy in small_loads:
            copy.wait()
        for l in range(layers):
            earlier(l)
        wo_loads[0].wait()
        send_weights()
        state_loads[0].wait()

    for l in range(layers):
        with jax.named_scope(f"in_wait{l}"):
            total_wait(in_recv.at[l], n_dp - 1, recv_sem.at[in_at(l)])
        mixer(l)
        with jax.named_scope(f"send_mix{l}"):
            send_mix(l)
            if l == 0:
                pl.semaphore_wait(know_sem.at[0], 2)
                for to in (2 * blocks, -2 * blocks):
                    signal(know_sem.at[1], tp_at(to))
                window(l)
                total_wait(wo_near, blocks - 1, recv_sem.at[weights_near])
                for copy in w_loads[1]:
                    copy.wait()
        with jax.named_scope(f"mix_wait{l}"):
            wait_mix(l, recv_sem.at[mix_at(l)])
        if l + 1 < layers:
            project(l + 1, reduce_all())
            with jax.named_scope(f"send_in{l + 1}"):
                send_in(l + 1)
                state_loads[l + 1].wait()
                wo_loads[l + 1].wait()
        else:
            reduce_rows(l)

    with jax.named_scope("end"):
        for l in range(layers):
            total_wait(in_send.at[l], n_dp - 1, send_sem.at[in_at(l)])
            wait_mix(l, send_sem.at[mix_at(l)])
        total_wait(wo_near, blocks - 1, send_sem.at[weights_near])
        total_wait(far_recv, far - 1, send_sem.at[far_sum])
        total_wait(pair_v, 1, send_sem.at[pair_sum])
        total_wait(own_recv, blocks - 1, send_sem.at[near_all])
        total_wait(part_send, n_tp - 1, send_sem.at[ring_sum])


def write_out(pieces, hidden_v, states_v, windows_v, hidden, states, windows, sem):
    copies = [
        pltpu.make_async_copy(hidden_v, hidden, sem.at[0]),
        pltpu.make_async_copy(windows_v, windows, sem.at[1]),
    ]
    layers, batch = states.shape[:2]
    step = layers * batch // pieces
    for p in range(pieces):
        l, b = divmod(p * step, batch)
        part = pl.ds(b, step)
        copies.append(
            pltpu.make_async_copy(states_v.at[l, part], states.at[l, part], sem.at[2 + p])
        )
    for copy in copies:
        copy.start()
    for copy in copies:
        copy.wait()


def body(n_tp, n_dp, *args):
    args = list(args)
    args[7] = jnp.transpose(args[7], (0, 2, 1))
    args[8] = jnp.transpose(args[8], (1, 2, 0, 3))
    args[9] = jnp.transpose(args[9], (0, 1, 3, 2, 4))
    args[13] = jnp.transpose(args[13], (0, 2, 1))
    h, w_value, history, state, w_out = (args[k] for k in (0, 3, 9, 14, 16))
    layers, feats, chans = w_value.shape
    batch = h.shape[0]
    rows = batch // n_dp
    roles, width_back = history.shape[2:4]
    blocks = feats // LANES
    vmem = pl.BlockSpec(memory_space=pltpu.VMEM)
    hbm = pl.BlockSpec(memory_space=pl.ANY)
    kept = pltpu.VMEM((batch // n_tp, feats), BF16), pltpu.VMEM(state.shape, F32), pltpu.VMEM(
        history.shape, BF16
    )
    in_vmem = pl.pallas_call(
        functools.partial(kernel, n_tp, n_dp),
        out_shape=kept,
        in_specs=[hbm] * len(args),
        out_specs=(vmem, vmem, vmem),
        scratch_shapes=[
            pltpu.SMEM(args[1].shape, args[1].dtype),
            *(pltpu.VMEM(args[k].shape, args[k].dtype) for k in (2, 7, 8)),
            *(pltpu.SMEM(args[k].shape, args[k].dtype) for k in (10, 11, 12)),
            *(pltpu.VMEM(args[k].shape, args[k].dtype) for k in (13, 15)),
            pltpu.VMEM((batch, feats), BF16),
            pltpu.VMEM((layers, feats, 4 * chans), BF16),
            pltpu.VMEM(w_out.shape, BF16),
            pltpu.VMEM(history.shape, BF16),
            pltpu.VMEM(state.shape, F32),
            pltpu.VMEM((rows * roles * width_back, LANES), F32),
            pltpu.VMEM((layers, rows * roles * width_back, LANES), F32),
            pltpu.VMEM((layers, roles, rows, LANES), F32),
            pltpu.VMEM((layers, 4, rows, LANES), F32),
            pltpu.VMEM((n_tp * 8, LANES), F32),
            pltpu.VMEM((layers, n_dp, 5, rows, LANES), BF16),
            pltpu.VMEM((layers, n_dp, 5, rows, LANES), BF16),
            pltpu.VMEM((n_dp, rows, LANES), BF16),
            pltpu.VMEM((blocks * n_dp, rows, LANES), BF16),
            pltpu.VMEM((blocks, chans, LANES), BF16),
            pltpu.VMEM((2, batch, LANES), BF16),
            pltpu.VMEM((n_tp // (2 * blocks), batch, LANES), BF16),
            pltpu.VMEM((blocks, batch, LANES), BF16),
            pltpu.VMEM((n_tp, 8, LANES), BF16),
            pltpu.VMEM((n_tp, 8, LANES), BF16),
            pltpu.SemaphoreType.DMA((3 + 3 * layers,)),
            pltpu.SemaphoreType.DMA((2 * layers + 5,)),
            pltpu.SemaphoreType.DMA((2 * layers + 5,)),
            pltpu.SemaphoreType.REGULAR((2,)),
        ],
        compiler_params=pltpu.CompilerParams(collective_id=0, has_side_effects=True),
    )(*args)
    pieces = 4
    hidden, states, windows = pl.pallas_call(
        functools.partial(write_out, pieces),
        out_shape=tuple(jax.ShapeDtypeStruct(k.shape, k.dtype) for k in in_vmem),
        in_specs=[vmem] * 3,
        out_specs=(hbm, hbm, hbm),
        scratch_shapes=[pltpu.SemaphoreType.DMA((2 + pieces,))],
    )(*(pltpu.with_memory_space_constraint(k, pltpu.VMEM) for k in in_vmem))
    return hidden, states, jnp.transpose(windows, (0, 1, 3, 2, 4))


def solution(mesh):
    placed = (
        P("grp", "dp"),
        P(("grp", "dp")),
        P(None, "dp"),
        P(None, "dp", "tp"),
        P(None, "dp", "tp"),
        P(None, "dp", "tp"),
        P(None, "dp", "tp"),
        P(None, "dp", None),
        P(None, None, None, "tp"),
        P(None, ("grp", "dp"), None, None, "tp"),
        P(None, "tp"),
        P(None, "tp"),
        P(None, "tp"),
        P(None, ("grp", "dp"), "tp"),
        P(None, ("grp", "dp"), "tp", None, None),
        P(None, "tp"),
        P(None, "tp", "dp"),
    )
    return jax.shard_map(
        functools.partial(body, mesh.shape["tp"], mesh.shape["dp"]),
        mesh=mesh,
        in_specs=placed,
        out_specs=(
            P(("grp", "tp"), "dp"),
            P(None, ("grp", "dp"), "tp", None, None),
            P(None, ("grp", "dp"), None, None, "tp"),
        ),
        check_vma=False,
    )
```

```python
import functools

import jax
import jax.numpy as jnp
from jax import lax
from jax.experimental import pallas as pl
from jax.experimental.pallas import tpu as pltpu
from jax.sharding import PartitionSpec as P

D = 4096
EPSILON = 1e-06
MESH = pl.DeviceIdType.MESH
F32 = jnp.float32
BF16 = jnp.bfloat16
LANES = 128
STAT = 3
SPACING = 2000


def total_wait(buffer, count, sem):
    part = buffer.at[pl.ds(0, count)]
    pltpu.make_async_copy(part, part, sem).wait()


def kernel(
    n_tp,
    n_dp,
    h_in,
    counts_in,
    in_gain_in,
    w_value,
    w_inkey,
    w_readkey,
    w_gate,
    w_step_in,
    taps_in,
    history,
    step_bias_in,
    decay_log_in,
    direct_gain_in,
    extra_log_in,
    state_in,
    out_gain_in,
    w_out,
    hidden_out,
    state_out,
    window_out,
    counts,
    in_gain,
    w_step,
    taps,
    step_bias,
    decay_log,
    direct_gain,
    extra_log,
    out_gain,
    h_v,
    wp_v,
    wo_v,
    hist_v,
    state_v,
    hist_f,
    win_f,
    early_v,
    fixed_v,
    tile_f,
    in_send,
    in_recv,
    mix_recv,
    wide_recv,
    wo_near,
    pair_v,
    far_recv,
    own_recv,
    part_send,
    part_recv,
    load_sem,
    send_sem,
    recv_sem,
    know_sem,
):
    layers = w_out.shape[0]
    batch, feats = h_in.shape
    rows = batch // n_dp
    blocks = feats // LANES
    head_dim = state_in.shape[3]
    heads = state_in.shape[2]
    roles, width_back = history.shape[2:4]
    far = n_tp // (2 * blocks)
    me_tp = lax.axis_index("tp")
    me_dp = lax.axis_index("dp")
    me_block = me_tp // blocks
    me_quarter = lax.rem(me_tp, blocks)
    me_pair = me_block // 2
    odd = lax.rem(me_block, 2)

    def tp_at(shift):
        return {"tp": lax.rem(me_tp + (n_tp + shift), n_tp)}

    def dp_at(shift):
        return {"dp": lax.rem(me_dp + shift, n_dp)}

    near = [
        blocks - 1 - me_quarter,
        me_quarter + 2 - 4 * (me_quarter // 2),
        me_quarter + 1 - 2 * lax.rem(me_quarter, 2),
    ]
    assert blocks == len(near) + 1

    def near_at(quarter):
        return {"tp": me_block * blocks + quarter}

    def remote(source, target, sem, to):
        pltpu.make_async_remote_copy(
            src_ref=source,
            dst_ref=target,
            send_sem=send_sem.at[sem],
            recv_sem=recv_sem.at[sem],
            device_id=to,
            device_id_type=MESH,
        ).start()

    def signal(sem, to):
        pl.semaphore_signal(sem, inc=1, device_id=to, device_id_type=MESH)

    in_at = lambda l: l
    mix_at = lambda l: layers + l
    weights_near, far_sum, near_all, ring_sum, pair_sum = (2 * layers + k for k in range(5))
    dp_shifts = sorted(range(1, n_dp), key=lambda s: abs(s - n_dp // 2))

    def load(source, target, sem):
        copy = pltpu.make_async_copy(source, target, load_sem.at[sem])
        copy.start()
        return copy

    def load_products(l):
        return [
            load(w.at[l], wp_v.at[l, :, pl.ds(k * LANES, LANES)], 1 + l)
            for k, w in enumerate((w_value, w_inkey, w_readkey, w_gate))
        ]

    h_load = [load(h_in, h_v, 0), load(in_gain_in, in_gain, 0)]
    w_loads = [load_products(0)]
    step_load = load(w_step_in, w_step, 1 + layers)

    barrier = pltpu.get_barrier_semaphore()
    for shift in range(1, n_dp):
        signal(barrier, dp_at(shift))
    for shift in range(1, blocks + 1):
        for to in (shift, -shift):
            signal(barrier, tp_at(to))

    lane = lax.broadcasted_iota(jnp.int32, (rows, LANES), 1)
    lane_all = lax.broadcasted_iota(jnp.int32, (batch, LANES), 1)
    sub = lax.broadcasted_iota(jnp.int32, (rows, LANES), 0)
    first_head = lane < head_dim
    unit = (
        lax.broadcasted_iota(jnp.int32, (LANES, LANES), 0)
        == lax.broadcasted_iota(jnp.int32, (LANES, LANES), 1)
    ).astype(BF16)

    def halves(x):
        high = x.astype(BF16)
        return high, (x - high.astype(F32)).astype(BF16)

    def spread(values, in_layer):
        return jnp.where(first_head, values[in_layer, 0], values[in_layer, 1])

    def project(l, h):
        with jax.named_scope(f"proj{l}"):
            squares = jnp.sum(h * h, axis=1, keepdims=True)
            scaled = (h * in_gain[l : l + 1, :]).astype(BF16)
            if l == 0:
                step_load.wait()
            steps = lax.dot_general(
                scaled, w_step[l], (((1,), (1,)), ((), ())), preferred_element_type=F32
            )
            lane_step = lax.broadcasted_iota(jnp.int32, steps.shape, 1)
            wanted = [
                jnp.sum(
                    jnp.where(lane_step == me_tp * heads + k, steps, 0.0), axis=1, keepdims=True
                )
                for k in range(heads)
            ] + [squares]
            if l == 0:
                for copy in w_loads[l]:
                    copy.wait()
            part = jnp.dot(scaled, wp_v[l], preferred_element_type=F32)
            stats = jnp.zeros((batch, LANES), F32)
            for k, v in enumerate(wanted):
                high = v.astype(BF16).astype(F32)
                stats = jnp.where(lane_all == k, high, stats)
                stats = jnp.where(lane_all == k + STAT, v - high, stats)
            for i in range(n_dp):
                at = slice(i * rows, (i + 1) * rows)
                for k in range(4):
                    in_send[l, i, k] = part[at, k * LANES : (k + 1) * LANES].astype(BF16)
                in_send[l, i, 4] = stats[at].astype(BF16)

    def send_in(l):
        for shift in dp_shifts:
            to = dp_at(shift)
            remote(in_send.at[l, to["dp"]], in_recv.at[l, me_dp], in_at(l), to)
        in_recv[l, me_dp] = in_send[l, me_dp]

    def earlier(l):
        lens = jnp.zeros((rows, LANES), jnp.int32)
        for b in range(rows):
            lens = jnp.where(sub == b, counts[b], lens)
        for b in range(rows):
            for r in range(roles):
                hist_f[pl.ds((b * roles + r) * width_back, width_back), :] = hist_v[
                    l, b, r
                ].astype(F32)
        for r in range(roles):
            total = jnp.zeros((rows, LANES), F32)
            for j in range(width_back):
                past = hist_f[pl.ds(r * width_back + j, rows, stride=roles * width_back), :]
                live = jnp.where(lens >= width_back - j, past, 0.0)
                total = total + live * taps[j, r, l : l + 1].astype(F32)
                if j:
                    win_f[
                        l, pl.ds(r * width_back + j - 1, rows, stride=roles * width_back), :
                    ] = past
            early_v[l, r] = total
        diagonal = lax.broadcasted_iota(jnp.int32, (rows, rows), 0) == lax.broadcasted_iota(
            jnp.int32, (rows, rows), 1
        )
        extra = [
            jnp.sum(jnp.where(diagonal, extra_log[l, k : k + 1, :], 0.0), axis=1, keepdims=True)
            for k in range(heads)
        ]
        fixed_v[l, 0] = jnp.where(first_head, extra[0], extra[1])
        fixed_v[l, 1] = jnp.exp(spread(decay_log, l))
        fixed_v[l, 2] = spread(step_bias, l)
        fixed_v[l, 3] = spread(direct_gain, l)

    def window(l):
        for b in range(rows):
            for r in range(roles):
                window_out[l, b, r] = win_f[
                    l, pl.ds((b * roles + r) * width_back, width_back), :
                ].astype(BF16)

    def mixer(l):
        with jax.named_scope(f"mixer{l}"):
            arrived = jnp.sum(in_recv[l].astype(F32), axis=0)
            stats = arrived[4]

            def stat(k):
                both = jnp.where((lane == k) | (lane == k + STAT), stats, 0.0)
                return jnp.sum(both, axis=1, keepdims=True)

            inverse = lax.rsqrt(stat(heads) / D + EPSILON)
            current = [(inverse * arrived[k]).astype(BF16).astype(F32) for k in range(roles)]
            gate = (inverse * arrived[3]).astype(BF16).astype(F32)
            step = jnp.where(first_head, stat(0), stat(1)) * inverse
            step = step.astype(BF16).astype(F32)
            value, inkey, readkey = [
                jax.nn.silu(
                    early_v[l, r] + current[r] * taps[width_back, r, l : l + 1].astype(F32)
                )
                for r in range(roles)
            ]
            rate = jax.nn.softplus(step + fixed_v[l, 2])
            decay = jnp.exp(-rate * fixed_v[l, 1] + fixed_v[l, 0])
            gain = rate * value
            high, low = halves(gain)
            none = jnp.zeros((rows, LANES), F32)
            parts = jnp.concatenate([high, high, low, none.astype(BF16)], axis=0)
            columns = lax.dot_general(
                unit, parts, (((1,), (1,)), ((), ())), preferred_element_type=F32
            ).astype(BF16)
            high, low = (half.astype(F32) for half in halves(inkey))
            right = jnp.concatenate(
                [
                    jnp.concatenate(
                        [jnp.where(sub == b, half, 0.0) for half in (high, low, high)] + [none],
                        axis=0,
                    )
                    for b in range(rows)
                ],
                axis=1,
            ).astype(BF16)
            outer = jnp.dot(columns, right, preferred_element_type=F32)
            reader = readkey.astype(BF16)
            fades = [
                jnp.broadcast_to(decay[:, k * head_dim : k * head_dim + 1], (rows, LANES))
                for k in range(heads)
            ]
            readout = jnp.zeros((rows, LANES), F32)
            for b in range(rows):
                news = []
                for k in range(heads):
                    added = outer[
                        k * head_dim : (k + 1) * head_dim, b * LANES : (b + 1) * LANES
                    ]
                    new = fades[k][b : b + 1] * state_v[l, b, k] + added
                    state_out[l, b, k] = new
                    news.append(new.astype(BF16))
                read = lax.dot_general(
                    reader,
                    jnp.concatenate(news, axis=0),
                    (((1,), (1,)), ((), ())),
                    preferred_element_type=F32,
                )
                readout = jnp.where(sub == b, read, readout)
            readout = readout + fixed_v[l, 3] * value
            gated = readout * jax.nn.silu(gate)
            scale = lax.rsqrt(jnp.mean(gated * gated, axis=1, keepdims=True) + EPSILON)
            normed = (gated * scale * out_gain[l : l + 1, :]).astype(BF16)
            if l + 1 < layers:
                wide_recv[me_quarter * n_dp + me_dp] = normed
            else:
                mix_recv[me_dp] = normed
            for r in range(roles):
                win_f[
                    l, pl.ds((r + 1) * width_back - 1, rows, stride=roles * width_back), :
                ] = current[r]

    def send_mix(l):
        if l + 1 < layers:
            here = wide_recv.at[me_quarter * n_dp + me_dp]
            for shift in dp_shifts:
                for quarter in near:
                    remote(here, here, mix_at(l), near_at(quarter) | dp_at(shift))
            for quarter in near:
                remote(here, here, mix_at(l), near_at(quarter))
        else:
            here = mix_recv.at[me_dp]
        for shift in dp_shifts:
            remote(here, here, mix_at(l), dp_at(shift))

    def wait_mix(l, sem):
        if l + 1 < layers:
            total_wait(wide_recv, blocks * n_dp - 1, sem)
        else:
            total_wait(mix_recv, n_dp - 1, sem)

    def send_weights():
        for quarter in near:
            columns = pl.ds(pl.multiple_of(quarter * LANES, LANES), LANES)
            remote(wo_v.at[0, :, columns], wo_near.at[me_quarter], weights_near, near_at(quarter))
        columns = pl.ds(pl.multiple_of(me_quarter * LANES, LANES), LANES)
        wo_near[me_quarter] = wo_v[0, :, columns]

    def reduce_all():
        with jax.named_scope("far_send"):
            mix = jnp.concatenate(
                [
                    jnp.concatenate(
                        [wide_recv[q * n_dp + i].astype(F32) for i in range(n_dp)], axis=0
                    ).astype(BF16)
                    for q in range(blocks)
                ],
                axis=1,
            )
            part = jnp.dot(
                mix, wo_near[...].reshape(-1, LANES), preferred_element_type=F32
            )
            pair_v[0] = part.astype(BF16)
            remote(pair_v.at[0], pair_v.at[1], pair_sum, {"tp": me_tp + blocks - 2 * blocks * odd})
            h = h_v[:, pl.ds(pl.multiple_of(me_quarter * LANES, LANES), LANES)].astype(F32)
        with jax.named_scope("pair_wait"):
            total_wait(pair_v, 1, recv_sem.at[pair_sum])
        with jax.named_scope("pair_send"):
            far_recv[me_pair] = (pair_v[0].astype(F32) + pair_v[1].astype(F32)).astype(BF16)
            pl.semaphore_wait(know_sem.at[1], 2)
            for step in range(far - 1, 0, -1):
                if step < far - 1:
                    pl.delay(SPACING)
                away = step * blocks * (2 * odd - 1)
                to = {"tp": lax.rem(me_tp + n_tp + away, n_tp)}
                remote(far_recv.at[me_pair], far_recv.at[me_pair], far_sum, to)
        with jax.named_scope("far_wait"):
            total_wait(far_recv, far - 1, recv_sem.at[far_sum])
        with jax.named_scope("near_all"):
            mine = (h + jnp.sum(far_recv[...].astype(F32), axis=0)).astype(BF16)
            own_recv[me_quarter] = mine
            for n, quarter in enumerate(near):
                if n:
                    pl.delay(SPACING // 3)
                remote(own_recv.at[me_quarter], own_recv.at[me_quarter], near_all, near_at(quarter))
        with jax.named_scope("near_all_wait"):
            total_wait(own_recv, blocks - 1, recv_sem.at[near_all])
        return jnp.concatenate([own_recv[j].astype(F32) for j in range(blocks)], axis=1)

    def reduce_rows(l):
        with jax.named_scope("ring_send"):
            kept_rows = batch // n_tp
            mix = jnp.concatenate(
                [mix_recv[i].astype(F32) for i in range(n_dp)], axis=0
            ).astype(BF16)
            part = jnp.dot(mix, wo_v[l], preferred_element_type=F32)
            for j in range(blocks):
                tile_f[pl.ds(j, batch, stride=blocks), :] = part[:, j * LANES : (j + 1) * LANES]
            for i in range(n_tp):
                part_send[i] = tile_f[i * 8 : (i + 1) * 8, :].astype(BF16)

            def to(shift):
                at = lax.rem(me_tp + shift, n_tp)
                remote(part_send.at[at], part_recv.at[me_tp], ring_sum, {"tp": at})

            def pair(step, _):
                to(n_tp // 2 - step)
                to(n_tp // 2 + step)
                return 0

            to(n_tp // 2)
            lax.fori_loop(1, n_tp // 2, pair, 0)
            part_recv[me_tp] = part_send[me_tp]
        with jax.named_scope("ring_wait"):
            at_row = lax.broadcasted_iota(jnp.int32, (8, batch), 0)
            at_col = lax.broadcasted_iota(jnp.int32, (8, batch), 1)
            pick = ((at_col == kept_rows * me_tp + at_row) & (at_row < kept_rows)).astype(BF16)
            h = jnp.concatenate([own_recv[j] for j in range(blocks)], axis=1)
            kept = jnp.dot(pick, h, preferred_element_type=F32)[0:kept_rows]
            window(l)
            total_wait(part_recv, n_tp - 1, recv_sem.at[ring_sum])
        with jax.named_scope("ring_sum"):
            tile_f[0:8, :] = jnp.sum(part_recv[...].astype(F32), axis=0)
            update = jnp.concatenate(
                [tile_f[pl.ds(j, kept_rows, stride=blocks), :] for j in range(blocks)], axis=1
            )
            hidden_out[...] = (kept + update).astype(BF16)

    with jax.named_scope("load_wait"):
        for copy in h_load:
            copy.wait()
    project(0, h_v[...].astype(F32))
    with jax.named_scope("barrier"):
        pl.semaphore_wait(barrier, n_dp - 1 + 2 * blocks)
    with jax.named_scope("send_in0"):
        send_in(0)
        for to in (blocks, -blocks):
            signal(know_sem.at[0], tp_at(to))
        small_loads = [
            load(source, target, 2 + layers)
            for source, target in (
                (history, hist_v),
                (counts_in, counts),
                (taps_in, taps),
                (step_bias_in, step_bias),
                (decay_log_in, decay_log),
                (direct_gain_in, direct_gain),
                (extra_log_in, extra_log),
                (out_gain_in, out_gain),
            )
        ]
        state_loads = [load(state_in.at[0], state_v.at[0], 3 + layers)]
        wo_loads = [load(w_out.at[0], wo_v.at[0], 3 + 2 * layers)]
        for l in range(1, layers):
            w_loads.append(load_products(l))
            state_loads.append(load(state_in.at[l], state_v.at[l], 3 + layers + l))
            wo_loads.append(load(w_out.at[l], wo_v.at[l], 3 + 2 * layers + l))
        for copy in small_loads:
            copy.wait()
        for l in range(layers):
            earlier(l)
        wo_loads[0].wait()
        send_weights()
        state_loads[0].wait()

    for l in range(layers):
        with jax.named_scope(f"in_wait{l}"):
            total_wait(in_recv.at[l], n_dp - 1, recv_sem.at[in_at(l)])
        mixer(l)
        with jax.named_scope(f"send_mix{l}"):
            send_mix(l)
            if l == 0:
                pl.semaphore_wait(know_sem.at[0], 2)
                for to in (2 * blocks, -2 * blocks):
                    signal(know_sem.at[1], tp_at(to))
                window(l)
                total_wait(wo_near, blocks - 1, recv_sem.at[weights_near])
                for copy in w_loads[1]:
                    copy.wait()
        with jax.named_scope(f"mix_wait{l}"):
            wait_mix(l, recv_sem.at[mix_at(l)])
        if l + 1 < layers:
            project(l + 1, reduce_all())
            with jax.named_scope(f"send_in{l + 1}"):
                send_in(l + 1)
                state_loads[l + 1].wait()
                wo_loads[l + 1].wait()
        else:
            reduce_rows(l)

    with jax.named_scope("end"):
        for l in range(layers):
            total_wait(in_send.at[l], n_dp - 1, send_sem.at[in_at(l)])
            wait_mix(l, send_sem.at[mix_at(l)])
        total_wait(wo_near, blocks - 1, send_sem.at[weights_near])
        total_wait(far_recv, far - 1, send_sem.at[far_sum])
        total_wait(pair_v, 1, send_sem.at[pair_sum])
        total_wait(own_recv, blocks - 1, send_sem.at[near_all])
        total_wait(part_send, n_tp - 1, send_sem.at[ring_sum])


def write_out(pieces, hidden_v, states_v, windows_v, hidden, states, windows, sem):
    copies = [
        pltpu.make_async_copy(hidden_v, hidden, sem.at[0]),
        pltpu.make_async_copy(windows_v, windows, sem.at[1]),
    ]
    layers, batch = states.shape[:2]
    step = layers * batch // pieces
    for p in range(pieces):
        l, b = divmod(p * step, batch)
        part = pl.ds(b, step)
        copies.append(
            pltpu.make_async_copy(states_v.at[l, part], states.at[l, part], sem.at[2 + p])
        )
    for copy in copies:
        copy.start()
    for copy in copies:
        copy.wait()


def body(n_tp, n_dp, *args):
    args = list(args)
    args[7] = jnp.transpose(args[7], (0, 2, 1))
    args[8] = jnp.transpose(args[8], (1, 2, 0, 3))
    args[9] = jnp.transpose(args[9], (0, 1, 3, 2, 4))
    args[13] = jnp.transpose(args[13], (0, 2, 1))
    h, w_value, history, state, w_out = (args[k] for k in (0, 3, 9, 14, 16))
    layers, feats, chans = w_value.shape
    batch = h.shape[0]
    rows = batch // n_dp
    roles, width_back = history.shape[2:4]
    blocks = feats // LANES
    vmem = pl.BlockSpec(memory_space=pltpu.VMEM)
    hbm = pl.BlockSpec(memory_space=pl.ANY)
    kept = pltpu.VMEM((batch // n_tp, feats), BF16), pltpu.VMEM(state.shape, F32), pltpu.VMEM(
        history.shape, BF16
    )
    in_vmem = pl.pallas_call(
        functools.partial(kernel, n_tp, n_dp),
        out_shape=kept,
        in_specs=[hbm] * len(args),
        out_specs=(vmem, vmem, vmem),
        scratch_shapes=[
            pltpu.SMEM(args[1].shape, args[1].dtype),
            *(pltpu.VMEM(args[k].shape, args[k].dtype) for k in (2, 7, 8)),
            *(pltpu.SMEM(args[k].shape, args[k].dtype) for k in (10, 11, 12)),
            *(pltpu.VMEM(args[k].shape, args[k].dtype) for k in (13, 15)),
            pltpu.VMEM((batch, feats), BF16),
            pltpu.VMEM((layers, feats, 4 * chans), BF16),
            pltpu.VMEM(w_out.shape, BF16),
            pltpu.VMEM(history.shape, BF16),
            pltpu.VMEM(state.shape, F32),
            pltpu.VMEM((rows * roles * width_back, LANES), F32),
            pltpu.VMEM((layers, rows * roles * width_back, LANES), F32),
            pltpu.VMEM((layers, roles, rows, LANES), F32),
            pltpu.VMEM((layers, 4, rows, LANES), F32),
            pltpu.VMEM((n_tp * 8, LANES), F32),
            pltpu.VMEM((layers, n_dp, 5, rows, LANES), BF16),
            pltpu.VMEM((layers, n_dp, 5, rows, LANES), BF16),
            pltpu.VMEM((n_dp, rows, LANES), BF16),
            pltpu.VMEM((blocks * n_dp, rows, LANES), BF16),
            pltpu.VMEM((blocks, chans, LANES), BF16),
            pltpu.VMEM((2, batch, LANES), BF16),
            pltpu.VMEM((n_tp // (2 * blocks), batch, LANES), BF16),
            pltpu.VMEM((blocks, batch, LANES), BF16),
            pltpu.VMEM((n_tp, 8, LANES), BF16),
            pltpu.VMEM((n_tp, 8, LANES), BF16),
            pltpu.SemaphoreType.DMA((3 + 3 * layers,)),
            pltpu.SemaphoreType.DMA((2 * layers + 5,)),
            pltpu.SemaphoreType.DMA((2 * layers + 5,)),
            pltpu.SemaphoreType.REGULAR((2,)),
        ],
        compiler_params=pltpu.CompilerParams(collective_id=0, has_side_effects=True),
    )(*args)
    pieces = 4
    hidden, states, windows = pl.pallas_call(
        functools.partial(write_out, pieces),
        out_shape=tuple(jax.ShapeDtypeStruct(k.shape, k.dtype) for k in in_vmem),
        in_specs=[vmem] * 3,
        out_specs=(hbm, hbm, hbm),
        scratch_shapes=[pltpu.SemaphoreType.DMA((2 + pieces,))],
    )(*(pltpu.with_memory_space_constraint(k, pltpu.VMEM) for k in in_vmem))
    return hidden, states, jnp.transpose(windows, (0, 1, 3, 2, 4))


def solution(mesh):
    placed = (
        P("grp", "dp"),
        P(("grp", "dp")),
        P(None, "dp"),
        P(None, "dp", "tp"),
        P(None, "dp", "tp"),
        P(None, "dp", "tp"),
        P(None, "dp", "tp"),
        P(None, "dp", None),
        P(None, None, None, "tp"),
        P(None, ("grp", "dp"), None, None, "tp"),
        P(None, "tp"),
        P(None, "tp"),
        P(None, "tp"),
        P(None, ("grp", "dp"), "tp"),
        P(None, ("grp", "dp"), "tp", None, None),
        P(None, "tp"),
        P(None, "tp", "dp"),
    )
    return jax.shard_map(
        functools.partial(body, mesh.shape["tp"], mesh.shape["dp"]),
        mesh=mesh,
        in_specs=placed,
        out_specs=(
            P(("grp", "tp"), "dp"),
            P(None, ("grp", "dp"), "tp", None, None),
            P(None, ("grp", "dp"), None, None, "tp"),
        ),
        check_vma=False,
    )
```
